512 devices in a mesh: ep: 128 (over z, x, core), tp: 4 (over y).
Axes of the slice: x: 4, y: 4, z: 16, core: 2. Of those that a mesh axis runs over, the one named last changes fastest.
Arguments:
- tokens: bfloat16 [16384, 1024], P('ep', 'tp'), may hold values from -6 to 6
- cotangent: bfloat16 [16384, 1024], P('ep', 'tp'), may hold values from -12 to 12
- routes: int32 [16384, 2], P('ep'), may hold values from 0 to 63, all different within a row; in each aligned block of 128 rows (0 to 127, 128 to 255, ...) at most 5 rows name the same one
- route_weights: bfloat16 [16384, 2], P('ep'), may hold values from 0.099609375 to 0.8984375
- w_gate: bfloat16 [128, 1024, 1408], P('ep', None, 'tp'), may hold values from -0.1875 to 0.1875
- w_up: bfloat16 [128, 1024, 1408], P('ep', None, 'tp'), may hold values from -0.1875 to 0.1875
- w_down: bfloat16 [128, 1408, 1024], P('ep', 'tp'), may hold values from -0.109375 to 0.109375
- dense_weight: bfloat16 [1024, 1024], P('tp', 'ep'), may hold values from -0.75 to 0.75
- mix_gate: float32 [1024], replicated, may hold values from 0.1 to 1.9
Outputs:
- token_grad: bfloat16 [16384, 1024], P('ep', 'tp')
- route_grad: float32 [16384, 2], P('ep')
- gate_grad: bfloat16 [128, 1024, 1408], P('ep', None, 'tp')
- up_grad: bfloat16 [128, 1024, 1408], P('ep', None, 'tp')
- down_grad: bfloat16 [128, 1408, 1024], P('ep', 'tp')
- dense_grad: float32 [1024, 1024], P('tp', 'ep')
- mix_grad: float32 [1024], replicated
The draws below stay inside these ranges and needn't reach their ends.
Inputs may be any that keep to these rules, and one draw needn't show every extreme that they name: `routes`: each row names 2 different experts. In the rows of one index of ep (aligned blocks of 128 rows) no expert is named by more than 5 rows, a bound that some block reaches.
All inputs are finite; a program needn't handle non-finite values.
Results may differ from the reference program's by a relative error of at most 0.0065.
Values may be sent and summed in bfloat16 or wider, within the bound.
A program may use at most 64 MiB of HBM per device.

```python
import math
import jax
import jax.numpy as jnp
import numpy as np
from jax import lax

D = 1024
FF = 2816
TOP = 2
TOK_DEV = 128
GROUP = 2
EXPERTS = 64
CAP = 5
FFB = 1408
SLICE = 352
TOKENS = 16384
N_EP = 128
N_TP = 4


def strengthened(values, stream_key, source, target, shards_of, factor):
    owner, partner = [(jnp.arange(values.shape[axis_at]) // (values.shape[axis_at] // shards_of)).reshape([-1 if axis == axis_at else 1 for axis in range(values.ndim)]) for axis_at in (source, target)]
    chosen = jax.random.permutation(stream_key, shards_of)[partner]
    strong = (owner == chosen) | (owner == (partner + shards_of // 2) % shards_of)
    return jnp.where(strong, factor * values, values)


def block_scale(stream_key, dims, pieces, smallest, top_value):
    factor_of, own = 1.0, jax.random.fold_in(stream_key, 6)
    for dim, blocks in pieces:
        draws = jnp.exp(jax.random.uniform(jax.random.fold_in(own, dim), (blocks,), jnp.float32, smallest / len(pieces), top_value / len(pieces)))
        factor_of = factor_of * jnp.repeat(draws, dims[dim] // blocks).reshape([-1 if axis == dim else 1 for axis in range(len(dims))])
    return factor_of


def deal_out(own_key, own, number, rows, number_of, top, limit, lean):
    sequence = jax.random.permutation(own_key, number_of)
    packed, ordinary = shares(number_of, rows * top, limit, lean, True), shares(number_of, rows * top, limit, lean, False)
    places = jnp.arange(number_of)

    def named(sizes, offset_by):
        used = int((sizes > 0).sum())
        fixed = max(1, used // 4)
        passed = fixed + (places - fixed + offset_by * (used - fixed)) % max(1, number_of - fixed)
        return jnp.zeros((number_of,), jnp.int32).at[sequence[jnp.where(places < fixed, places, passed)]].set(jnp.asarray(sizes, jnp.int32))

    sizes = jnp.where(number % 4 == 0, named(packed, number // 4), named(ordinary, number - number // 4 - 1))
    mixed = jax.random.permutation(jax.random.fold_in(own, 3), number_of)
    donor, taker = mixed[0:number_of // 2 * 2:2], mixed[1:number_of // 2 * 2:2]
    room = jnp.minimum(sizes[donor] - 1, limit - sizes[taker]) // 2
    room = jnp.where((donor == sequence[0]) | (taker == sequence[0]) | (sizes[taker] == 0), 0, jnp.maximum(room, 0))
    passed = jax.random.randint(jax.random.fold_in(own, 4), (number_of // 2,), 0, 1 << 20) % (room + 1)
    sizes = sizes.at[donor].add(-passed).at[taker].add(passed)
    labels = jnp.searchsorted(jnp.cumsum(sizes), jnp.arange(rows * top), side="right").astype(jnp.int32)
    listing = labels.reshape(top, rows).T
    listing = listing[jax.random.permutation(jax.random.fold_in(own, 1), rows)]
    offset_by = jax.random.randint(jax.random.fold_in(own, 2), (rows, 1), 0, top)
    return jnp.take_along_axis(listing, (jnp.arange(top)[None, :] + offset_by) % top, axis=1)


def shares(amount, total, limit, lean, full):
    loads = [(1 << 20) // math.isqrt(rank ** lean) + 1 for rank in range(1, amount + 1)]
    largest = limit if full else min(limit, max(-(-total // amount), total * loads[0] // sum(loads)))
    least = 1 if total - largest >= amount - 1 else 0
    counts, surplus = [largest] + [least] * (amount - 1), total - largest - least * (amount - 1)
    while surplus > 0:
        movable = [i for i in range(1, amount) if counts[i] < largest] or [i for i in range(1, amount) if counts[i] < limit]
        mass, left = sum([loads[i] for i in movable]), surplus
        for i in movable:
            extra = min(limit - counts[i], max(1, left * loads[i] // mass), surplus)
            counts[i] = counts[i] + extra
            surplus = surplus - extra
    return np.array(counts)


def noise(key, dims, scale, most, shards=(), held_as=jnp.bfloat16):
    drawn = scale * jax.random.normal(key, dims, jnp.float32)
    if shards:
        drawn = drawn * block_scale(key, dims, shards, -0.22, 0.18)
    return jnp.clip(drawn, -most, most).astype(held_as)


def noise_with(own_key, extent, width, most, cuts, heavy, kind=jnp.bfloat16):
    values = width * jax.random.normal(own_key, extent, jnp.float32)
    if cuts:
        values = values * block_scale(own_key, extent, cuts, -0.22, 0.18)
    return jnp.clip(strengthened(values, jax.random.fold_in(own_key, 3), *heavy), -most, most).astype(kind)


def setup_inputs(seed: int = 0) -> dict:
    streams_of = jax.random.split(jax.random.key(seed), 10)
    tokens = noise(streams_of[0], (TOKENS, D), 1.0, 6.0, ((0, 128), (1, 4)))
    cotangent = noise_with(streams_of[1], (TOKENS, D), 0.5, 12.0, ((0, 128), (1, 4)), (0, 1, 128, 5.5))
    routes_keys = jax.random.split(jax.random.fold_in(streams_of[2], 1), TOKENS // TOK_DEV)
    routes_turns = jax.random.permutation(jax.random.fold_in(streams_of[2], 3), TOKENS // TOK_DEV)
    routes = jax.vmap(lambda own, number: deal_out(jax.random.fold_in(streams_of[2], 2), own, number, TOK_DEV, EXPERTS, TOP, CAP, 2))(routes_keys, routes_turns).reshape((TOKENS, TOP))
    route_weights = jnp.clip(0.099609375 + 0.7988281 * jax.random.uniform(streams_of[3], (TOKENS, TOP), jnp.float32) ** block_scale(streams_of[3], (TOKENS, TOP), ((0, 128),), -0.2, 0.2), 0.099609375, 0.8984375).astype(jnp.bfloat16)
    w_gate = noise(streams_of[4], (EXPERTS * GROUP, D, FFB), D ** -0.5, 0.1875, ((0, 128), (2, 4)))
    w_up = noise(streams_of[5], (EXPERTS * GROUP, D, FFB), D ** -0.5, 0.1875, ((0, 128), (2, 4)))
    w_down = noise(streams_of[6], (EXPERTS * GROUP, FFB, D), FF ** -0.5, 0.109375, ((0, 128), (1, 4)))
    dense_weight = noise_with(streams_of[7], (D, D), D ** -0.5, 0.75, ((0, 4), (1, 128)), (1, 0, 128, 5.5))
    mix_gate = jnp.clip(1.0 + 0.18 * jax.random.normal(streams_of[8], (D,), jnp.float32), 0.1, 1.9)
    return dict(tokens=tokens, cotangent=cotangent, routes=routes, route_weights=route_weights, w_gate=w_gate, w_up=w_up, w_down=w_down, dense_weight=dense_weight, mix_gate=mix_gate)


def reference(tokens, cotangent, routes, route_weights, w_gate, w_up, w_down, dense_weight, mix_gate):
    picks = TOK_DEV * TOP
    slots = EXPERTS * CAP
    blocked = routes.reshape(N_EP, picks)
    onehot = (blocked[:, :, None] == jnp.arange(EXPERTS, dtype=jnp.int32)[None, None, :]).astype(jnp.int32)
    ranking = jnp.cumsum(onehot, axis=1) - 1
    target = (blocked * CAP + jnp.sum(onehot * ranking, axis=2)).astype(jnp.int32)
    pick_index = jnp.arange(picks, dtype=jnp.int32)
    block_base = (jnp.arange(N_EP, dtype=jnp.int32) * TOK_DEV)[:, None]
    token_index = (block_base + pick_index[None, :] // TOP).astype(jnp.int32)
    block_rows = jnp.broadcast_to(jnp.arange(N_EP, dtype=jnp.int32)[:, None], target.shape)
    source = jnp.zeros((N_EP, slots), jnp.int32).at[block_rows, target].set(token_index)
    pick_slot = jnp.zeros((N_EP, slots), jnp.int32).at[block_rows, target].set(
        jnp.broadcast_to(pick_index[None, :] % TOP, target.shape).astype(jnp.int32))
    filled = jnp.zeros((N_EP, slots), jnp.float32).at[block_rows, target].set(1.0)
    slot_weight = jnp.zeros((N_EP, slots), jnp.float32).at[block_rows, target].set(
        route_weights.reshape(N_EP, picks).astype(jnp.float32))

    def by_expert(table):
        return table.reshape(N_EP, EXPERTS, CAP).transpose(1, 0, 2).reshape(EXPERTS, N_EP * CAP)

    gate_blocks = w_gate.reshape(EXPERTS, GROUP, D, FFB)
    up_blocks = w_up.reshape(EXPERTS, GROUP, D, FFB)
    down_blocks = w_down.reshape(EXPERTS, GROUP, FFB, D)
    slices = GROUP * N_TP

    def one_expert(carry, inputs):
        token_acc, route_acc = carry
        src, kslot, live, weight, gate_b, up_b, down_b = inputs
        token_rows = tokens[src]
        grad_rows = cotangent[src]
        gate_matrix = gate_b.transpose(1, 0, 2).reshape(D, FF)
        up_matrix = up_b.transpose(1, 0, 2).reshape(D, FF)
        down_matrix = down_b.reshape(FF, D)
        pre_gate = jnp.dot(token_rows, gate_matrix, preferred_element_type=jnp.float32)
        pre_up = jnp.dot(token_rows, up_matrix, preferred_element_type=jnp.float32)
        sigmoid_gate = jax.nn.sigmoid(pre_gate)
        activated = pre_gate * sigmoid_gate
        hidden = activated * pre_up
        hidden_bf = hidden.astype(jnp.bfloat16)
        projected = jnp.dot(grad_rows, down_matrix.T, preferred_element_type=jnp.float32)
        route_part = jnp.sum(hidden_bf.astype(jnp.float32) * projected, axis=1)
        weight_col = weight[:, None]
        hidden_grad = weight_col * projected
        d_gate = (hidden_grad * pre_up * sigmoid_gate * (1.0 + pre_gate * (1.0 - sigmoid_gate))).astype(jnp.bfloat16)
        d_up = (hidden_grad * activated).astype(jnp.bfloat16)
        weighted = (weight_col * hidden).astype(jnp.bfloat16)
        gate_delta = jnp.dot(token_rows.T, d_gate, preferred_element_type=jnp.float32).astype(jnp.bfloat16)
        up_delta = jnp.dot(token_rows.T, d_up, preferred_element_type=jnp.float32).astype(jnp.bfloat16)
        down_delta = jnp.dot(weighted.T, grad_rows, preferred_element_type=jnp.float32).astype(jnp.bfloat16)
        row_count = token_rows.shape[0]
        gate_slices = d_gate.astype(jnp.float32).reshape(row_count, slices, SLICE)
        up_slices = d_up.astype(jnp.float32).reshape(row_count, slices, SLICE)
        gate_cols = gate_matrix.astype(jnp.float32).reshape(D, slices, SLICE)
        up_cols = up_matrix.astype(jnp.float32).reshape(D, slices, SLICE)
        partial_value = (jnp.einsum('rsf,dsf->rsd', gate_slices, gate_cols)
                   + jnp.einsum('rsf,dsf->rsd', up_slices, up_cols)).astype(jnp.bfloat16)
        block_sum = jnp.sum(partial_value.reshape(row_count, GROUP, N_TP, D).astype(jnp.float32), axis=2).astype(jnp.bfloat16)
        summed = jnp.sum(block_sum.astype(jnp.float32), axis=1)
        token_acc = token_acc.at[src].add(summed * live[:, None])
        route_acc = route_acc.at[src, kslot].add(route_part * live)
        outputs = (gate_delta.reshape(D, GROUP, FFB).transpose(1, 0, 2),
                   up_delta.reshape(D, GROUP, FFB).transpose(1, 0, 2),
                   down_delta.reshape(GROUP, FFB, D))
        return (token_acc, route_acc), outputs

    start = (jnp.zeros((TOKENS, D), jnp.float32), jnp.zeros((TOKENS, TOP), jnp.float32))
    inputs = (by_expert(source), by_expert(pick_slot), by_expert(filled), by_expert(slot_weight),
              gate_blocks, up_blocks, down_blocks)
    (token_acc, route_acc), (gate_all, up_all, down_all) = lax.scan(one_expert, start, inputs)
    scaled = (mix_gate[None, :] * cotangent.astype(jnp.float32)).astype(jnp.bfloat16)
    dense_dx = jnp.dot(scaled, dense_weight.T, preferred_element_type=jnp.float32)
    token_grad = (token_acc + dense_dx).astype(jnp.bfloat16)
    dense_grad = jnp.dot(tokens.T, scaled, preferred_element_type=jnp.float32) / N_EP
    dense_out = jnp.dot(tokens, dense_weight, preferred_element_type=jnp.float32)
    mix_grad = jnp.sum(cotangent.astype(jnp.float32) * dense_out, axis=0) / N_EP
    gate_grad = gate_all.reshape(EXPERTS * GROUP, D, FFB)
    up_grad = up_all.reshape(EXPERTS * GROUP, D, FFB)
    down_grad = down_all.reshape(EXPERTS * GROUP, FFB, D)
    return token_grad, route_acc, gate_grad, up_grad, down_grad, dense_grad, mix_grad
```

```python
import jax
import jax.numpy as jnp
from jax import lax
from jax.experimental import pallas as pl
from jax.experimental.pallas import tpu as pltpu
from jax.sharding import Mesh
from jax.sharding import PartitionSpec as P

EP = ("z", "x", "c")
MESH = pl.DeviceIdType.MESH
BF = jnp.bfloat16
F32 = jnp.float32
NZ = 16
NX = 4
NC = 2
NY = 4
CAP = 5
EXPERTS = NZ * NX
HK = NZ // NC
NQ = NX * NC
BLK = NQ * CAP
Z_ORDER = (0, 1, 7, 2, 6, 3, 5, 4)


def rdma(src, dst, send, recv, device):
    return pltpu.make_async_remote_copy(
        src_ref=src, dst_ref=dst, send_sem=send, recv_sem=recv, device_id=device, device_id_type=MESH
    )


def where_am_i():
    return tuple(lax.axis_index(a) for a in ("z", "x", "c", "y"))


def enter():
    z, x, c, y = where_am_i()
    barrier = pltpu.get_barrier_semaphore()

    def greet(device):
        pl.semaphore_signal(barrier, inc=1, device_id=device, device_id_type=MESH)

    for step in range(1, NQ):
        other = lax.rem(c * NX + x + step, NQ)
        greet((z, lax.rem(other, NX), other // NX, y))
    for step in range(1, NZ):
        greet((lax.rem(z + step, NZ), x, c, y))
    for step in range(1, NY):
        greet((z, x, c, lax.rem(y + step, NY)))
    pl.semaphore_wait(barrier, NQ - 1 + NZ - 1 + NY - 1)


def cols(index, width):
    return pl.ds(pl.multiple_of(index * width, width), width)


def permuted(perm_ref, value_ref, out_ref):
    width = value_ref.shape[-1]
    flat = value_ref[...].reshape(NQ * BLK, width)
    moved = jnp.dot(perm_ref[...], flat, preferred_element_type=F32).astype(BF)
    out_ref[...] = moved.reshape(NQ, BLK, width)


def dispatch_kernel(
    tok_ref, cot_slot_ref, cot_ref, wt_ref, perm_ref,
    rows_ref, grads_ref, full_ref, dense_ref,
    x_tok, x_cot, p_tok, p_cot,
    local_sem, x_send, x_recv, z_send, z_recv, yp_send, yp_recv, ym_send, ym_recv, f_send, f_recv,
    c_send, c_recv, g_send, g_recv, dz_send, dz_recv, dx_send, dx_recv, dc_send, dc_recv,
):
    z, x, c, y = where_am_i()
    width = tok_ref.shape[-1]
    me_q = c * NX + x
    y_up, y_down = lax.rem(y + 1, NY), lax.rem(y + NY - 1, NY)
    y_far = lax.rem(y + 2, NY)
    partner = (z, x, 1 - c, y)
    slots = (tok_ref, cot_slot_ref)
    gathered = (x_tok, x_cot)
    sorted_rows = (p_tok, p_cot)
    outs = (rows_ref, grads_ref)

    own = [
        pltpu.make_async_copy(tok_ref.at[me_q], x_tok.at[me_q], local_sem.at[0]),
        pltpu.make_async_copy(cot_slot_ref.at[me_q], x_cot.at[me_q], local_sem.at[1]),
        pltpu.make_async_copy(cot_ref, full_ref.at[:, cols(y, width)], local_sem.at[2]),
        pltpu.make_async_copy(wt_ref, dense_ref.at[z, x, c], local_sem.at[3]),
    ]
    for copy in own:
        copy.start()
    enter()

    def x_copy(a, step):
        other = lax.rem(me_q + step, NQ)
        return rdma(
            slots[a].at[other], gathered[a].at[me_q], x_send.at[a, step], x_recv.at[a, step],
            (z, lax.rem(other, NX), other // NX, y),
        )

    def x_arrival(a, step):
        source = lax.rem(me_q + NQ - step, NQ)
        return rdma(
            slots[a].at[source], gathered[a].at[source], x_send.at[a, step], x_recv.at[a, step],
            (z, lax.rem(source, NX), source // NX, y),
        )

    for a in range(2):
        for step in range(1, NQ):
            x_copy(a, step).start()

    def g_copy(step):
        return rdma(
            cot_ref, full_ref.at[:, cols(y, width)], g_send.at[step], g_recv.at[step],
            (z, x, c, lax.rem(y + step, NY)),
        )

    def g_arrival(step):
        source = lax.rem(y + NY - step, NY)
        return rdma(
            cot_ref, full_ref.at[:, cols(source, width)], g_send.at[step], g_recv.at[step],
            (z, x, c, source),
        )

    for step in range(1, NY):
        g_copy(step).start()

    def dz_copy(step):
        return rdma(
            wt_ref, dense_ref.at[z, x, c], dz_send.at[step], dz_recv.at[step],
            (lax.rem(z + step, NZ), x, c, y),
        )

    def dz_arrival(step):
        source = lax.rem(z + NZ - step, NZ)
        return rdma(
            wt_ref, dense_ref.at[source, x, c], dz_send.at[step], dz_recv.at[step], (source, x, c, y)
        )

    @pl.loop(1, NZ)
    def _(step):
        dz_copy(step).start()

    def z_copy(a, k):
        target = lax.rem(z + 2 * k + c, NZ)
        return rdma(
            sorted_rows[a].at[k], outs[a].at[c * HK + k, :, cols(y, width)],
            z_send.at[a, k], z_recv.at[a, k], (target, x, c, y),
        )

    def z_home(a):
        return pltpu.make_async_copy(
            sorted_rows[a].at[0], outs[a].at[0, :, cols(y, width)], local_sem.at[4 + a]
        )

    for a in range(2):
        own[a].wait()
        for step in range(1, NQ):
            x_arrival(a, step).wait_recv()
        permuted(perm_ref, gathered[a], sorted_rows[a])
        for k in Z_ORDER:
            if k == 0:

                @pl.when(c == 0)
                def _():
                    z_home(a).start()

                @pl.when(c == 1)
                def _():
                    z_copy(a, 0).start()
            else:
                z_copy(a, k).start()

    def y_copy(a, k, up):
        part = outs[a].at[c * HK + k, :, cols(y, width)]
        if up:
            return rdma(part, part, yp_send.at[a, k], yp_recv.at[a, k], (z, x, c, y_up))
        return rdma(part, part, ym_send.at[a, k], ym_recv.at[a, k], (z, x, c, y_down))

    def y_arrival(a, k, up):
        if up:
            part = outs[a].at[c * HK + k, :, cols(y_down, width)]
            return rdma(part, part, yp_send.at[a, k], yp_recv.at[a, k], (z, x, c, y_down))
        part = outs[a].at[c * HK + k, :, cols(y_up, width)]
        return rdma(part, part, ym_send.at[a, k], ym_recv.at[a, k], (z, x, c, y_up))

    def f_copy(a, k):
        source, target = (y_down, y_up) if k % 2 == 0 else (y_up, y_down)
        part = outs[a].at[c * HK + k, :, cols(source, width)]
        return rdma(part, part, f_send.at[a, k], f_recv.at[a, k], (z, x, c, target))

    def f_arrival(a, k):
        part = outs[a].at[c * HK + k, :, cols(y_far, width)]
        return rdma(part, part, f_send.at[a, k], f_recv.at[a, k], (z, x, c, y_up))

    def c_copy(a, k):
        block = outs[a].at[c * HK + k]
        return rdma(block, block, c_send.at[a, k], c_recv.at[a, k], partner)

    def c_arrival(a, k):
        block = outs[a].at[(1 - c) * HK + k]
        return rdma(block, block, c_send.at[a, k], c_recv.at[a, k], partner)

    def dx_copy(step):
        part = dense_ref.at[:, x, c]
        return rdma(part, part, dx_send.at[step], dx_recv.at[step], (z, lax.rem(x + step, NX), c, y))

    def dx_arrival(step):
        source = lax.rem(x + NX - step, NX)
        part = dense_ref.at[:, source, c]
        return rdma(part, part, dx_send.at[step], dx_recv.at[step], (z, source, c, y))

    def dc_copy(core):
        part = dense_ref.at[:, :, core]
        return rdma(part, part, dc_send.at[0], dc_recv.at[0], partner)

    order = [(a, k) for a in range(2) for k in Z_ORDER]
    for i in range(len(order) + 2):
        if i < len(order):
            a, k = order[i]
            if k == 0:

                @pl.when(c == 0)
                def _():
                    z_home(a).wait()

                @pl.when(c == 1)
                def _():
                    z_copy(a, 0).wait_recv()
            else:
                z_copy(a, k).wait_recv()
            y_copy(a, k, True).start()
            y_copy(a, k, False).start()
        if 1 <= i <= len(order):
            a, k = order[i - 1]
            up = k % 2 == 0
            y_arrival(a, k, up).wait_recv()
            f_copy(a, k).start()
            y_arrival(a, k, not up).wait_recv()
        if i >= 2:
            a, k = order[i - 2]
            f_arrival(a, k).wait_recv()
            c_copy(a, k).start()
        if i == 6:
            own[3].wait()

            @pl.loop(1, NZ)
            def _(step):
                dz_arrival(step).wait_recv()

            for step in range(1, NX):
                dx_copy(step).start()
        if i == 10:
            for step in range(1, NX):
                dx_arrival(step).wait_recv()
            dc_copy(c).start()

    own[2].wait()
    for step in range(1, NY):
        g_arrival(step).wait_recv()
    dc_copy(1 - c).wait_recv()
    for a, k in order:
        c_arrival(a, k).wait_recv()
    for a in range(2):
        for step in range(1, NQ):
            x_copy(a, step).wait_send()
    for step in range(1, NY):
        g_copy(step).wait_send()

    @pl.loop(1, NZ)
    def _(step):
        dz_copy(step).wait_send()

    for step in range(1, NX):
        dx_copy(step).wait_send()
    dc_copy(c).wait_send()
    for a, k in order:
        if k == 0:

            @pl.when(c == 1)
            def _():
                z_copy(a, 0).wait_send()
        else:
            z_copy(a, k).wait_send()
        y_copy(a, k, True).wait_send()
        y_copy(a, k, False).wait_send()
        f_copy(a, k).wait_send()
        c_copy(a, k).wait_send()


def combine_kernel(
    part_ref, aux_ref, moment_ref, gain_ref, perm_ref,
    out_ref, aux_out, moment_out, gain_out,
    p_in, aux_in, m_in, g_in,
    first, first_in, second_in, back, back_in, sorted_back,
    aux_sum, aux_y, aux_z, aux_t,
    m_half, m_x, m_xsum, m_z, g_sum, g_x, g_sum2, g_y, g_sum3, g_z,
    local_sem, d_send, d_recv, b1_send, b1_recv, b2_send, b2_recv, ay_send, ay_recv,
    z_send, z_recv, za_send, za_recv, x_send, x_recv, xa_send, xa_recv,
    mx_send, mx_recv, mz_send, mz_recv, gx_send, gx_recv, gy_send, gy_recv, gz_send, gz_recv,
):
    z, x, c, y = where_am_i()
    width = out_ref.shape[-1]
    half = HK // 2
    me_q = c * NX + x
    partner = (z, x, 1 - c, y)
    flip1 = y + 1 - 2 * lax.rem(y, 2)
    flip3 = NY - 1 - y
    flip2 = lax.rem(y + 2, NY)
    pairs = ((flip1, flip3), (flip3, flip1))

    enter()
    d_copies = [
        rdma(part_ref.at[pl.ds((1 - c) * HK, HK)], p_in, d_send.at[0], d_recv.at[0], partner),
        rdma(aux_ref.at[pl.ds((1 - c) * HK, HK)], aux_in, d_send.at[1], d_recv.at[1], partner),
        rdma(gain_ref, g_in, d_send.at[2], d_recv.at[2], partner),
        rdma(moment_ref.at[:, :, 1 - c], m_in, d_send.at[3], d_recv.at[3], partner),
    ]
    for copy in d_copies:
        copy.start()

    d_copies[0].wait_recv()

    def b1_copy(h):
        return rdma(
            first.at[h, pl.ds(2, 2)], first_in.at[h], b1_send.at[h], b1_recv.at[h],
            (z, x, c, pairs[h][0]),
        )

    def both(h, i, owner):
        for j in range(half):
            mine = part_ref[c * HK + h * half + j, :, cols(owner, width)].astype(F32)
            theirs = p_in[h * half + j, :, cols(owner, width)].astype(F32)
            first[h, i, j] = (mine + theirs).astype(BF)

    for h in range(2):
        both(h, 2, pairs[h][0])
        both(h, 3, flip2)
        b1_copy(h).start()
    for h in range(2):
        both(h, 0, y)
        both(h, 1, pairs[h][1])

    d_copies[1].wait_recv()
    aux_sum[...] = aux_ref[pl.ds(c * HK, HK)] + aux_in[...]

    def ay_copy(step):
        return rdma(aux_sum, aux_y.at[y], ay_send.at[step], ay_recv.at[step],
                    (z, x, c, lax.rem(y + step, NY)))

    def ay_arrival(step):
        source = lax.rem(y + NY - step, NY)
        return rdma(aux_sum, aux_y.at[source], ay_send.at[step], ay_recv.at[step], (z, x, c, source))

    for step in range(1, NY):
        ay_copy(step).start()
    aux_y[y] = aux_sum[...]

    d_copies[2].wait_recv()
    g_sum[...] = gain_ref[...] + g_in[...]
    g_x[x] = g_sum[...]

    def gx_copy(step):
        return rdma(g_sum, g_x.at[x], gx_send.at[step], gx_recv.at[step],
                    (z, lax.rem(x + step, NX), c, y))

    def gx_arrival(step):
        source = lax.rem(x + NX - step, NX)
        return rdma(g_sum, g_x.at[source], gx_send.at[step], gx_recv.at[step], (z, source, c, y))

    for step in range(1, NX):
        gx_copy(step).start()

    d_copies[3].wait_recv()
    for i in range(NX):
        m_half[:, i] = moment_ref[:, i, c] + m_in[:, i]

    def mx_copy(step):
        other = lax.rem(x + step, NX)
        return rdma(m_half.at[:, other], m_x.at[step - 1], mx_send.at[step], mx_recv.at[step],
                    (z, other, c, y))

    for step in range(1, NX):
        mx_copy(step).start()

    def b2_copy(h):
        return rdma(first.at[h, 3], second_in.at[h], b2_send.at[h], b2_recv.at[h],
                    (z, x, c, pairs[h][1]))

    for h in range(2):
        b1_copy(h).wait()
        first[h, 3] = (first[h, 1].astype(F32) + first_in[h, 1].astype(F32)).astype(BF)
        b2_copy(h).start()

    for step in range(1, NX):
        gx_arrival(step).wait_recv()
    g_sum2[...] = g_x[0] + g_x[1] + g_x[2] + g_x[3]
    g_y[y] = g_sum2[...]

    def gy_copy(step):
        return rdma(g_sum2, g_y.at[y], gy_send.at[step], gy_recv.at[step],
                    (z, x, c, lax.rem(y + step, NY)))

    def gy_arrival(step):
        source = lax.rem(y + NY - step, NY)
        return rdma(g_sum2, g_y.at[source], gy_send.at[step], gy_recv.at[step], (z, x, c, source))

    for step in range(1, NY):
        gy_copy(step).start()

    for step in range(1, NX):
        mx_copy(step).wait_recv()
    m_xsum[...] = m_half[:, x] + m_x[0] + m_x[1] + m_x[2]

    def mz_copy(step):
        other = lax.rem(z + step, NZ)
        return rdma(m_xsum.at[other], m_z.at[step], mz_send.at[step], mz_recv.at[step],
                    (other, x, c, y))

    @pl.loop(1, NZ)
    def _(step):
        mz_copy(step).start()

    for step in range(1, NY):
        ay_arrival(step).wait_recv()
        ay_copy(step).wait_send()
    aux_sum[...] = aux_y[0] + aux_y[1] + aux_y[2] + aux_y[3]

    def z_copy(k):
        target = lax.rem(z + 2 * NZ - 2 * k - c, NZ)
        return rdma(back.at[k], back_in.at[k], z_send.at[k], z_recv.at[k], (target, x, c, y))

    def za_copy(k):
        target = lax.rem(z + 2 * NZ - 2 * k - c, NZ)
        return rdma(aux_sum.at[k], aux_z.at[k], za_send.at[k], za_recv.at[k], (target, x, c, y))

    z_home = [
        pltpu.make_async_copy(back.at[0], back_in.at[0], local_sem.at[0]),
        pltpu.make_async_copy(aux_sum.at[0], aux_z.at[0], local_sem.at[1]),
    ]

    def send_back(k):
        if k == 0:

            @pl.when(c == 0)
            def _():
                z_home[0].start()
                z_home[1].start()

            @pl.when(c == 1)
            def _():
                z_copy(0).start()
                za_copy(0).start()
        else:
            z_copy(k).start()
            za_copy(k).start()

    for h in range(2):
        b2_copy(h).wait()
        back[pl.ds(h * half, half)] = (
            first[h, 0].astype(F32) + first_in[h, 0].astype(F32) + second_in[h].astype(F32)
        ).astype(BF)
    for k in reversed(Z_ORDER):
        send_back(k)

    for step in range(1, NY):
        gy_arrival(step).wait_recv()
    g_sum3[...] = g_y[0] + g_y[1] + g_y[2] + g_y[3]
    g_z[z] = g_sum3[...]

    def gz_copy(step):
        return rdma(g_sum3, g_z.at[z], gz_send.at[step], gz_recv.at[step],
                    (lax.rem(z + step, NZ), x, c, y))

    def gz_arrival(step):
        source = lax.rem(z + NZ - step, NZ)
        return rdma(g_sum3, g_z.at[source], gz_send.at[step], gz_recv.at[step], (source, x, c, y))

    @pl.loop(1, NZ)
    def _(step):
        gz_copy(step).start()

    for k in Z_ORDER:
        if k == 0:

            @pl.when(c == 0)
            def _():
                z_home[0].wait()
                z_home[1].wait()

            @pl.when(c == 1)
            def _():
                z_copy(0).wait()
                za_copy(0).wait()
        else:
            z_copy(k).wait()
            za_copy(k).wait()
    permuted(perm_ref, back_in, sorted_back)
    for q in range(NQ):
        aux_t[q] = aux_z[:, q, :]

    def x_copy(step):
        other = lax.rem(me_q + step, NQ)
        return rdma(sorted_back.at[other], out_ref.at[me_q], x_send.at[step], x_recv.at[step],
                    (z, lax.rem(other, NX), other // NX, y))

    def xa_copy(step):
        other = lax.rem(me_q + step, NQ)
        return rdma(aux_t.at[other], aux_out.at[me_q], xa_send.at[step], xa_recv.at[step],
                    (z, lax.rem(other, NX), other // NX, y))

    def x_arrival(step):
        source = lax.rem(me_q + NQ - step, NQ)
        device = (z, lax.rem(source, NX), source // NX, y)
        return (
            rdma(sorted_back.at[source], out_ref.at[source], x_send.at[step], x_recv.at[step], device),
            rdma(aux_t.at[source], aux_out.at[source], xa_send.at[step], xa_recv.at[step], device),
        )

    for step in range(1, NQ):
        x_copy(step).start()
        xa_copy(step).start()
    out_ref[me_q] = sorted_back[me_q]
    aux_out[me_q] = aux_t[me_q]

    m_z[0] = m_xsum[z]

    @pl.loop(1, NZ)
    def _(step):
        mz_copy(step).wait()
        gz_arrival(step).wait_recv()
        gz_copy(step).wait_send()

    moment_out[...] = jnp.sum(m_z[...], axis=0)
    gain_out[...] = jnp.sum(g_z[...], axis=0)

    for step in range(1, NQ):
        for arrival in x_arrival(step):
            arrival.wait_recv()
        x_copy(step).wait_send()
        xa_copy(step).wait_send()
    for copy in d_copies:
        copy.wait_send()
    for step in range(1, NX):
        gx_copy(step).wait_send()
        mx_copy(step).wait_send()
    for step in range(1, NY):
        gy_copy(step).wait_send()


VMEM_SPEC = pl.BlockSpec(memory_space=pltpu.VMEM)
DMA = pltpu.SemaphoreType.DMA


def dispatch(tok_slots, cot_slots, cotangent, wt, perm):
    width = cotangent.shape[1]
    return pl.pallas_call(
        dispatch_kernel,
        out_shape=(
            jax.ShapeDtypeStruct((NZ, BLK, NY * width), BF),
            jax.ShapeDtypeStruct((NZ, BLK, NY * width), BF),
            jax.ShapeDtypeStruct((cotangent.shape[0], NY * width), BF),
            jax.ShapeDtypeStruct((NZ, NX, NC) + wt.shape, BF),
        ),
        in_specs=[VMEM_SPEC] * 5,
        out_specs=(VMEM_SPEC,) * 4,
        scratch_shapes=[pltpu.VMEM((NQ, BLK, width), BF)] * 4
        + [
            DMA((6,)),
            DMA((2, NQ)), DMA((2, NQ)),
            DMA((2, HK)), DMA((2, HK)),
            DMA((2, HK)), DMA((2, HK)),
            DMA((2, HK)), DMA((2, HK)),
            DMA((2, HK)), DMA((2, HK)),
            DMA((2, HK)), DMA((2, HK)),
            DMA((NY,)), DMA((NY,)),
            DMA((NZ,)), DMA((NZ,)),
            DMA((NX,)), DMA((NX,)),
            DMA((1,)), DMA((1,)),
        ],
        compiler_params=pltpu.CompilerParams(collective_id=0, has_side_effects=True),
        name="dispatch",
    )(tok_slots, cot_slots, cotangent, wt, perm)


def combine(partial, aux, moment, gain, perm):
    width = partial.shape[2] // NY
    half = HK // 2
    lanes = aux.shape[2]
    own, feats = moment.shape[3:]
    g = gain.shape
    vm = pltpu.VMEM
    return pl.pallas_call(
        combine_kernel,
        out_shape=(
            jax.ShapeDtypeStruct((NQ, BLK, width), BF),
            jax.ShapeDtypeStruct((NQ, HK, lanes), F32),
            jax.ShapeDtypeStruct((own, feats), F32),
            jax.ShapeDtypeStruct(g, F32),
        ),
        in_specs=[VMEM_SPEC] * 5,
        out_specs=(VMEM_SPEC,) * 4,
        scratch_shapes=[
            vm((HK, BLK, NY * width), BF),
            vm((HK, NQ, lanes), F32),
            vm((NZ, NX, own, feats), F32),
            vm(g, F32),
            vm((2, NY, half, BLK, width), BF),
            vm((2, 2, half, BLK, width), BF),
            vm((2, half, BLK, width), BF),
            vm((HK, BLK, width), BF),
            vm((HK, BLK, width), BF),
            vm((NQ, BLK, width), BF),
            vm((HK, NQ, lanes), F32),
            vm((NY, HK, NQ, lanes), F32),
            vm((HK, NQ, lanes), F32),
            vm((NQ, HK, lanes), F32),
            vm((NZ, NX, own, feats), F32),
            vm((NX - 1, NZ, own, feats), F32),
            vm((NZ, own, feats), F32),
            vm((NZ, own, feats), F32),
            vm(g, F32),
            vm((NX,) + g, F32),
            vm(g, F32),
            vm((NY,) + g, F32),
            vm(g, F32),
            vm((NZ,) + g, F32),
            DMA((2,)),
            DMA((4,)), DMA((4,)),
            DMA((2,)), DMA((2,)),
            DMA((2,)), DMA((2,)),
            DMA((NY,)), DMA((NY,)),
            DMA((HK,)), DMA((HK,)),
            DMA((HK,)), DMA((HK,)),
            DMA((NQ,)), DMA((NQ,)),
            DMA((NQ,)), DMA((NQ,)),
            DMA((NX,)), DMA((NX,)),
            DMA((NZ,)), DMA((NZ,)),
            DMA((NX,)), DMA((NX,)),
            DMA((NY,)), DMA((NY,)),
            DMA((NZ,)), DMA((NZ,)),
        ],
        compiler_params=pltpu.CompilerParams(collective_id=1, has_side_effects=True),
        name="combine",
    )(partial, aux, moment, gain, perm)


def local(tokens, cotangent, routes, route_weights, w_gate, w_up, w_down, dense_weight, mix_gate):
    z, x, c = (lax.axis_index(a) for a in EP)
    token_count = routes.shape[0]
    ep_count = NZ * NX * NC
    e = jnp.arange(EXPERTS, dtype=jnp.int32)
    expert = lax.rem(z + 2 * lax.rem(e, HK) + e // (HK * NX), NZ) * NX + lax.rem(e // HK, NX)
    picked = routes.T
    hits = [picked[p][None, :] == expert[:, None] for p in range(2)]
    hit = hits[0] | hits[1]
    t = jnp.arange(token_count, dtype=jnp.int32)
    earlier = (t[:, None] < t[None, :]).astype(BF)
    rank = jnp.dot(hit.astype(BF), earlier, preferred_element_type=F32).astype(jnp.int32)
    s = jnp.arange(CAP, dtype=jnp.int32)
    chosen = (hit[:, None, :] & (rank[:, None, :] == s[None, :, None])).reshape(-1, token_count)
    weights = route_weights.T
    weight = jnp.where(hits[0], weights[0][None, :], weights[1][None, :])
    weight = jnp.broadcast_to(weight[:, None, :], (EXPERTS, CAP, token_count)).reshape(-1, token_count)
    select = chosen.astype(BF)
    select_weighted = jnp.where(chosen, weight, jnp.zeros_like(weight))
    tok_slots = jnp.dot(select, tokens, preferred_element_type=F32).astype(BF).reshape(NQ, BLK, -1)
    cot_slots = (
        jnp.dot(select_weighted, cotangent, preferred_element_type=F32).astype(BF).reshape(NQ, BLK, -1)
    )
    r = jnp.arange(NQ * BLK, dtype=jnp.int32)
    moved = lax.rem(r, BLK) // CAP * BLK + r // BLK * CAP + lax.rem(r, CAP)
    perm = (moved[:, None] == r[None, :]).astype(BF)
    rows_in, grads_in, cot_full, wt_full = dispatch(
        tok_slots, cot_slots, cotangent, dense_weight.T, perm
    )

    rows_in = rows_in.reshape(NZ * BLK, -1)
    grads_in = grads_in.reshape(NZ * BLK, -1)
    wt_full = wt_full.reshape(ep_count * dense_weight.shape[1], -1)
    gate_matrix, up_matrix, down_matrix = w_gate[0], w_up[0], w_down[0]
    rows_by = (((0,), (0,)), ((), ()))
    cols_by = (((1,), (1,)), ((), ()))

    def dot(a, b, dims):
        return lax.dot_general(a, b, dims, preferred_element_type=F32)

    pre_gate = jnp.dot(rows_in, gate_matrix, preferred_element_type=F32)
    pre_up = jnp.dot(rows_in, up_matrix, preferred_element_type=F32)
    back = dot(grads_in, down_matrix, cols_by)
    sig = jax.nn.sigmoid(pre_gate)
    act = pre_gate * sig
    hidden_bf = (act * pre_up).astype(BF)
    route_part = jnp.sum(hidden_bf.astype(F32) * back, axis=1)
    d_gate = (back * pre_up * sig * (1.0 + pre_gate * (1.0 - sig))).astype(BF)
    d_up = (back * act).astype(BF)
    partial = (dot(d_gate, gate_matrix, cols_by) + dot(d_up, up_matrix, cols_by)).astype(BF)
    aux = jnp.pad(route_part.reshape(NZ, NQ, CAP), ((0, 0), (0, 0), (0, 128 - CAP)))
    moment = dot(cot_full, tokens, rows_by)
    gain = jnp.sum(wt_full.astype(F32) * moment, axis=1).reshape(-1, 128)
    own = dense_weight.shape[1]
    slots, aux_back, moment_own, gain_all = combine(
        partial.reshape(NZ, BLK, -1), aux, moment.reshape(NZ, NX, NC, own, -1), gain, perm
    )

    gate_grad = dot(rows_in, d_gate, rows_by).astype(BF)[None]
    up_grad = dot(rows_in, d_up, rows_by).astype(BF)[None]
    down_grad = dot(hidden_bf, grads_in, rows_by).astype(BF)[None]
    scaled = (mix_gate[None, :] * cot_full.astype(F32)).astype(BF)
    dense_dx = jnp.dot(scaled, wt_full, preferred_element_type=F32)
    token_grad = (dense_dx + dot(select, slots.reshape(NQ * BLK, -1), rows_by)).astype(BF)
    values = aux_back[:, :, :CAP].reshape(EXPERTS, CAP)
    at_slot = jnp.sum(
        jnp.where(rank[:, :, None] == s[None, None, :], values[:, None, :], 0.0), axis=2
    )
    route_sums = jnp.stack([jnp.sum(jnp.where(h, at_slot, 0.0), axis=0) for h in hits], axis=1)
    route_grad = route_sums / route_weights.astype(F32)
    ep_index = (z * NX + x) * NC + c
    own_gate = lax.dynamic_slice(mix_gate, (ep_index * own,), (own,))
    dense_grad = (moment_own * (own_gate[:, None] * (1.0 / ep_count))).T
    mix_grad = gain_all.reshape(-1) / ep_count
    return token_grad, route_grad, gate_grad, up_grad, down_grad, dense_grad, mix_grad


def solution(mesh):
    finer = Mesh(mesh.devices.reshape(NZ, NX, NC, NY), EP + ("y",))
    in_specs = (
        P(EP, "y"),
        P(EP, "y"),
        P(EP, None),
        P(EP, None),
        P(EP, None, "y"),
        P(EP, None, "y"),
        P(EP, "y", None),
        P("y", EP),
        P(),
    )
    out_specs = (
        P(EP, "y"),
        P(EP, None),
        P(EP, None, "y"),
        P(EP, None, "y"),
        P(EP, "y", None),
        P("y", EP),
        P(),
    )
    return jax.shard_map(local, mesh=finer, in_specs=in_specs, out_specs=out_specs, check_vma=False)
```

```python
import jax
import jax.numpy as jnp
from jax import lax
from jax.experimental import pallas as pl
from jax.experimental.pallas import tpu as pltpu
from jax.sharding import Mesh
from jax.sharding import PartitionSpec as P

EP = ("z", "x", "c")
MESH = pl.DeviceIdType.MESH
BF = jnp.bfloat16
F32 = jnp.float32
NZ = 16
NX = 4
NC = 2
NY = 4
CAP = 5
EXPERTS = NZ * NX
HK = NZ // NC
NQ = NX * NC
BLK = NQ * CAP
Z_ORDER = (0, 1, 7, 2, 6, 3, 5, 4)


def rdma(src, dst, send, recv, device):
    return pltpu.make_async_remote_copy(
        src_ref=src, dst_ref=dst, send_sem=send, recv_sem=recv, device_id=device, device_id_type=MESH
    )


def where_am_i():
    return tuple(lax.axis_index(a) for a in ("z", "x", "c", "y"))


def greet_all():
    z, x, c, y = where_am_i()
    barrier = pltpu.get_barrier_semaphore()

    def greet(device):
        pl.semaphore_signal(barrier, inc=1, device_id=device, device_id_type=MESH)

    for step in range(1, NQ):
        other = lax.rem(c * NX + x + step, NQ)
        greet((z, lax.rem(other, NX), other // NX, y))
    for step in range(1, NZ):
        greet((lax.rem(z + step, NZ), x, c, y))
    for step in range(1, NY):
        greet((z, x, c, lax.rem(y + step, NY)))


def wait_all():
    pl.semaphore_wait(pltpu.get_barrier_semaphore(), NQ - 1 + NZ - 1 + NY - 1)


def cols(index, width):
    return pl.ds(pl.multiple_of(index * width, width), width)


def permuted(perm_ref, value_ref, out_ref):
    width = value_ref.shape[-1]
    flat = value_ref[...].reshape(NQ * BLK, width)
    moved = jnp.dot(perm_ref[...], flat, preferred_element_type=F32).astype(BF)
    out_ref[...] = moved.reshape(NQ, BLK, width)


HALF = HK * BLK
LAG_F = 3
LAG_C = 6
PLAIN = (((1,), (0,)), ((), ()))
ROWS_BY = (((0,), (0,)), ((), ()))
COLS_BY = (((1,), (1,)), ((), ()))


def dot(a, b, dims):
    return lax.dot_general(a, b, dims, preferred_element_type=F32)


def gathered_rows(select_ref, value_ref):
    rows = dot(select_ref[...], value_ref[...], PLAIN).astype(BF)
    return rows.reshape(NQ, BLK, value_ref.shape[1])


def layer_kernel(
    sel_ref, selw_ref, tokens_ref, cot_ref, wt_ref, perm_ref, pick_ref, lane_ref,
    wg_hbm, wu_hbm, wd_hbm,
    out_ref, aux_out, moment_out, gain_out, full_ref, dense_ref, gate_out, up_out, down_out,
    *scratch,
):
    (
        s_tok, s_cot, x_tok, x_cot, p_tok, p_cot, rows_ref, grads_ref, wg, wu, wd, hid, dg, du,
        part, p_in, aux, aux_in, first, first_in, second_in, back, back_in, sorted_back, aux_sum,
        aux_y, aux_z, aux_t, moment_ref, m_in, m_half, m_x, m_xsum, m_z, g_mine, g_own, g_y,
        local_sem, x_send, x_recv, z_send, z_recv, yp_send, yp_recv, ym_send, ym_recv, f_send,
        f_recv, c_send, c_recv, g_send, g_recv, dz_send, dz_recv, dx_send, dx_recv, dc_send,
        dc_recv, mc_send, mc_recv, mx_send, mx_recv, mz_send, mz_recv, p_send, p_recv, b1_send,
        b1_recv, b2_send, b2_recv, ay_send, ay_recv, rz_send, rz_recv, rza_send, rza_recv, rx_send,
        rx_recv, rxa_send, rxa_recv, gy_send, gy_recv, gz_send, gz_recv, gx_send, gx_recv, gc_send,
        gc_recv,
    ) = scratch
    z, x, c, y = where_am_i()
    width = tokens_ref.shape[-1]
    me_q = c * NX + x
    y_up, y_down = lax.rem(y + 1, NY), lax.rem(y + NY - 1, NY)
    y_far = lax.rem(y + 2, NY)
    partner = (z, x, 1 - c, y)
    slots = (s_tok, s_cot)
    gathered = (x_tok, x_cot)
    sorted_rows = (p_tok, p_cot)
    outs = (rows_ref, grads_ref)

    own = [
        pltpu.make_async_copy(cot_ref, full_ref.at[:, cols(y, width)], local_sem.at[0]),
        pltpu.make_async_copy(wt_ref, dense_ref.at[z, x, c], local_sem.at[1]),
    ]
    for copy in own:
        copy.start()
    weights = [
        pltpu.make_async_copy(wg_hbm, wg, local_sem.at[6]),
        pltpu.make_async_copy(wu_hbm, wu, local_sem.at[7]),
        pltpu.make_async_copy(wd_hbm, wd, local_sem.at[8]),
    ]
    for copy in weights:
        copy.start()
    greet_all()
    slots[0][...] = gathered_rows(sel_ref, tokens_ref)
    slots[1][...] = gathered_rows(selw_ref, cot_ref)
    wait_all()

    def x_copy(a, step):
        other = lax.rem(me_q + step, NQ)
        return rdma(
            slots[a].at[other], gathered[a].at[me_q], x_send.at[a, step], x_recv.at[a, step],
            (z, lax.rem(other, NX), other // NX, y),
        )

    def x_arrival(a, step):
        source = lax.rem(me_q + NQ - step, NQ)
        return rdma(
            slots[a].at[source], gathered[a].at[source], x_send.at[a, step], x_recv.at[a, step],
            (z, lax.rem(source, NX), source // NX, y),
        )

    for a in range(2):
        for step in range(1, NQ):
            x_copy(a, step).start()

    def g_copy(step):
        return rdma(
            cot_ref, full_ref.at[:, cols(y, width)], g_send.at[step], g_recv.at[step],
            (z, x, c, lax.rem(y + step, NY)),
        )

    def g_arrival(step):
        source = lax.rem(y + NY - step, NY)
        return rdma(
            cot_ref, full_ref.at[:, cols(source, width)], g_send.at[step], g_recv.at[step],
            (z, x, c, source),
        )

    for step in range(1, NY):
        g_copy(step).start()

    def dz_copy(step):
        return rdma(
            wt_ref, dense_ref.at[z, x, c], dz_send.at[step], dz_recv.at[step],
            (lax.rem(z + step, NZ), x, c, y),
        )

    def dz_arrival(step):
        source = lax.rem(z + NZ - step, NZ)
        return rdma(
            wt_ref, dense_ref.at[source, x, c], dz_send.at[step], dz_recv.at[step], (source, x, c, y)
        )

    @pl.loop(1, NZ)
    def _(step):
        dz_copy(step).start()

    def z_copy(a, k):
        target = lax.rem(z + 2 * k + c, NZ)
        return rdma(
            sorted_rows[a].at[k], outs[a].at[c * HK + k, :, cols(y, width)],
            z_send.at[a, k], z_recv.at[a, k], (target, x, c, y),
        )

    def z_home(a):
        return pltpu.make_async_copy(
            sorted_rows[a].at[0], outs[a].at[0, :, cols(y, width)], local_sem.at[2 + a]
        )

    for a in range(2):
        gathered[a][me_q] = slots[a][me_q]
        for step in range(1, NQ):
            x_arrival(a, step).wait_recv()
        permuted(perm_ref, gathered[a], sorted_rows[a])
        for k in Z_ORDER:
            if k == 0:

                @pl.when(c == 0)
                def _():
                    z_home(a).start()

                @pl.when(c == 1)
                def _():
                    z_copy(a, 0).start()
            else:
                z_copy(a, k).start()

    def y_copy(a, k, up):
        part = outs[a].at[c * HK + k, :, cols(y, width)]
        if up:
            return rdma(part, part, yp_send.at[a, k], yp_recv.at[a, k], (z, x, c, y_up))
        return rdma(part, part, ym_send.at[a, k], ym_recv.at[a, k], (z, x, c, y_down))

    def y_arrival(a, k, up):
        if up:
            part = outs[a].at[c * HK + k, :, cols(y_down, width)]
            return rdma(part, part, yp_send.at[a, k], yp_recv.at[a, k], (z, x, c, y_down))
        part = outs[a].at[c * HK + k, :, cols(y_up, width)]
        return rdma(part, part, ym_send.at[a, k], ym_recv.at[a, k], (z, x, c, y_up))

    def f_copy(a, k):
        source, target = (y_down, y_up) if k % 2 == 0 else (y_up, y_down)
        part = outs[a].at[c * HK + k, :, cols(source, width)]
        return rdma(part, part, f_send.at[a, k], f_recv.at[a, k], (z, x, c, target))

    def f_arrival(a, k):
        part = outs[a].at[c * HK + k, :, cols(y_far, width)]
        return rdma(part, part, f_send.at[a, k], f_recv.at[a, k], (z, x, c, y_up))

    def c_copy(a, k):
        block = outs[a].at[c * HK + k]
        return rdma(block, block, c_send.at[a, k], c_recv.at[a, k], partner)

    def c_arrival(a, k):
        block = outs[a].at[(1 - c) * HK + k]
        return rdma(block, block, c_send.at[a, k], c_recv.at[a, k], partner)

    def dx_copy(step):
        part = dense_ref.at[:, x, c]
        return rdma(part, part, dx_send.at[step], dx_recv.at[step], (z, lax.rem(x + step, NX), c, y))

    def dx_arrival(step):
        source = lax.rem(x + NX - step, NX)
        part = dense_ref.at[:, source, c]
        return rdma(part, part, dx_send.at[step], dx_recv.at[step], (z, source, c, y))

    def dc_copy(core):
        part = dense_ref.at[:, :, core]
        return rdma(part, part, dc_send.at[0], dc_recv.at[0], partner)

    own[0].wait()
    for step in range(1, NY):
        g_arrival(step).wait_recv()
    moment_ref[...] = dot(full_ref[...], tokens_ref[...], ROWS_BY).reshape(moment_ref.shape)

    def mc_copy():
        return rdma(moment_ref.at[:, :, 1 - c], m_in, mc_send.at[0], mc_recv.at[0], partner)

    mc_copy().start()

    def mx_copy(step):
        other = lax.rem(x + step, NX)
        return rdma(m_half.at[:, other], m_x.at[step - 1], mx_send.at[step], mx_recv.at[step],
                    (z, other, c, y))

    def mz_copy(step):
        other = lax.rem(z + step, NZ)
        return rdma(m_xsum.at[other], m_z.at[step], mz_send.at[step], mz_recv.at[step],
                    (other, x, c, y))

    order = [(a, k) for a in range(2) for k in Z_ORDER]
    for i in range(len(order) + LAG_C):
        if i < len(order):
            a, k = order[i]
            if k == 0:

                @pl.when(c == 0)
                def _():
                    z_home(a).wait()

                @pl.when(c == 1)
                def _():
                    z_copy(a, 0).wait_recv()
            else:
                z_copy(a, k).wait_recv()
            y_copy(a, k, True).start()
            y_copy(a, k, False).start()
        if LAG_F <= i < len(order) + LAG_F:
            a, k = order[i - LAG_F]
            up = k % 2 == 0
            y_arrival(a, k, up).wait_recv()
            f_copy(a, k).start()
            y_arrival(a, k, not up).wait_recv()
        if i >= LAG_C:
            a, k = order[i - LAG_C]
            f_arrival(a, k).wait_recv()
            c_copy(a, k).start()
        if i == 6:
            own[1].wait()

            @pl.loop(1, NZ)
            def _(step):
                dz_arrival(step).wait_recv()

            for step in range(1, NX):
                dx_copy(step).start()
        if i == 8:
            mc_copy().wait_recv()
            for n in range(NX):
                m_half[:, n] = moment_ref[:, n, c] + m_in[:, n]
            for step in range(1, NX):
                mx_copy(step).start()
        if i == 12:
            for step in range(1, NX):
                dx_arrival(step).wait_recv()
            dc_copy(c).start()

    for step in range(1, NX):
        mx_copy(step).wait_recv()
    m_xsum[...] = m_half[:, x] + m_x[0] + m_x[1] + m_x[2]

    @pl.loop(1, NZ)
    def _(step):
        mz_copy(step).start()

    dc_copy(1 - c).wait_recv()
    for a, k in order:
        c_arrival(a, k).wait_recv()
    for copy in weights:
        copy.wait()

    def p_copy():
        return rdma(part.at[0], p_in, p_send.at[0], p_recv.at[0], partner)

    def pa_copy():
        return rdma(aux.at[0], aux_in, p_send.at[1], p_recv.at[1], partner)

    @pl.loop(0, 2)
    def _(turn):
        group = jnp.where(turn == 0, 1 - c, c)
        rows = rows_ref[pl.ds(group * HK, HK)].reshape(HALF, NY * width)
        grads = grads_ref[pl.ds(group * HK, HK)].reshape(HALF, NY * width)
        pre_gate = dot(rows, wg[...], PLAIN)
        pre_up = dot(rows, wu[...], PLAIN)
        back_h = dot(grads, wd[...], COLS_BY)
        sig = jax.nn.sigmoid(pre_gate)
        act = pre_gate * sig
        hidden_bf = (act * pre_up).astype(BF)
        hid[turn] = hidden_bf
        d_gate = (back_h * pre_up * sig * (1.0 + pre_gate * (1.0 - sig))).astype(BF)
        d_up = (back_h * act).astype(BF)
        dg[turn] = d_gate
        du[turn] = d_up
        route = jnp.sum(hidden_bf.astype(F32) * back_h, axis=1, keepdims=True)
        spread = route * lane_ref[...]
        high = spread.astype(BF)
        low = (spread - high.astype(F32)).astype(BF)
        placed = dot(pick_ref[...], high, PLAIN) + dot(pick_ref[...], low, PLAIN)
        aux[turn] = placed.reshape(HK, NQ, 128)
        both_parts = dot(d_gate, wg[...], COLS_BY) + dot(d_up, wu[...], COLS_BY)
        part[turn] = both_parts.astype(BF).reshape(HK, BLK, NY * width)

        @pl.when(turn == 0)
        def _():
            p_copy().start()
            pa_copy().start()

    half = HK // 2
    flip1 = y + 1 - 2 * lax.rem(y, 2)
    flip3 = NY - 1 - y
    flip2 = lax.rem(y + 2, NY)
    pairs = ((flip1, flip3), (flip3, flip1))

    p_copy().wait_recv()

    def b1_copy(h):
        return rdma(
            first.at[h, pl.ds(2, 2)], first_in.at[h], b1_send.at[h], b1_recv.at[h],
            (z, x, c, pairs[h][0]),
        )

    def both(h, i, owner):
        for j in range(half):
            mine = part[1, h * half + j, :, cols(owner, width)].astype(F32)
            theirs = p_in[h * half + j, :, cols(owner, width)].astype(F32)
            first[h, i, j] = (mine + theirs).astype(BF)

    for h in range(2):
        both(h, 2, pairs[h][0])
        both(h, 3, flip2)
        b1_copy(h).start()
    for h in range(2):
        both(h, 0, y)
        both(h, 1, pairs[h][1])

    pa_copy().wait_recv()
    aux_sum[...] = aux[1] + aux_in[...]

    def ay_copy(step):
        return rdma(aux_sum, aux_y.at[y], ay_send.at[step], ay_recv.at[step],
                    (z, x, c, lax.rem(y + step, NY)))

    def ay_arrival(step):
        source = lax.rem(y + NY - step, NY)
        return rdma(aux_sum, aux_y.at[source], ay_send.at[step], ay_recv.at[step], (z, x, c, source))

    for step in range(1, NY):
        ay_copy(step).start()
    aux_y[y] = aux_sum[...]

    def b2_copy(h):
        return rdma(first.at[h, 3], second_in.at[h], b2_send.at[h], b2_recv.at[h],
                    (z, x, c, pairs[h][1]))

    for h in range(2):
        b1_copy(h).wait()
        first[h, 3] = (first[h, 1].astype(F32) + first_in[h, 1].astype(F32)).astype(BF)
        b2_copy(h).start()

    m_z[0] = m_xsum[z]

    @pl.loop(1, NZ)
    def _(step):
        mz_copy(step).wait()

    moment_own = jnp.sum(m_z[...], axis=0)
    moment_out[...] = moment_own
    gain = jnp.sum(wt_ref[...].astype(F32) * moment_own, axis=1, keepdims=True)
    g_mine[...] = jnp.broadcast_to(gain, g_mine.shape)

    def gy_copy(step):
        return rdma(g_mine, g_y.at[y], gy_send.at[step], gy_recv.at[step],
                    (z, x, c, lax.rem(y + step, NY)))

    def gy_arrival(step):
        source = lax.rem(y + NY - step, NY)
        return rdma(g_mine, g_y.at[source], gy_send.at[step], gy_recv.at[step], (z, x, c, source))

    for step in range(1, NY):
        gy_copy(step).start()
    g_y[y] = g_mine[...]

    for step in range(1, NY):
        ay_arrival(step).wait_recv()
        ay_copy(step).wait_send()
    aux_sum[...] = aux_y[0] + aux_y[1] + aux_y[2] + aux_y[3]

    def r_z_copy(k):
        target = lax.rem(z + 2 * NZ - 2 * k - c, NZ)
        return rdma(back.at[k], back_in.at[k], rz_send.at[k], rz_recv.at[k], (target, x, c, y))

    def r_za_copy(k):
        target = lax.rem(z + 2 * NZ - 2 * k - c, NZ)
        return rdma(aux_sum.at[k], aux_z.at[k], rza_send.at[k], rza_recv.at[k], (target, x, c, y))

    r_z_home = [
        pltpu.make_async_copy(back.at[0], back_in.at[0], local_sem.at[4]),
        pltpu.make_async_copy(aux_sum.at[0], aux_z.at[0], local_sem.at[5]),
    ]

    def send_back(k):
        if k == 0:

            @pl.when(c == 0)
            def _():
                r_z_home[0].start()
                r_z_home[1].start()

            @pl.when(c == 1)
            def _():
                r_z_copy(0).start()
                r_za_copy(0).start()
        else:
            r_z_copy(k).start()
            r_za_copy(k).start()

    for h in range(2):
        b2_copy(h).wait()
        back[pl.ds(h * half, half)] = (
            first[h, 0].astype(F32) + first_in[h, 0].astype(F32) + second_in[h].astype(F32)
        ).astype(BF)
    for k in reversed(Z_ORDER):
        send_back(k)

    for step in range(1, NY):
        gy_arrival(step).wait_recv()
    g_own[...] = g_y[0] + g_y[1] + g_y[2] + g_y[3]

    def gz_copy(step):
        return rdma(g_own, gain_out.at[z, x, c], gz_send.at[step], gz_recv.at[step],
                    (lax.rem(z + step, NZ), x, c, y))

    def gz_arrival(step):
        source = lax.rem(z + NZ - step, NZ)
        return rdma(g_own, gain_out.at[source, x, c], gz_send.at[step], gz_recv.at[step],
                    (source, x, c, y))

    @pl.loop(1, NZ)
    def _(step):
        gz_copy(step).start()

    gain_out[z, x, c] = g_own[...]

    def over_rows(a, b):
        return dot(a, b, ROWS_BY)

    grows = (rows_ref[pl.ds((1 - c) * HK, HK)].reshape(HALF, NY * width), rows_ref[pl.ds(c * HK, HK)].reshape(HALF, NY * width))
    ggrads = (grads_ref[pl.ds((1 - c) * HK, HK)].reshape(HALF, NY * width), grads_ref[pl.ds(c * HK, HK)].reshape(HALF, NY * width))
    gate_out[...] = (over_rows(grows[0], dg[0]) + over_rows(grows[1], dg[1])).astype(BF)
    up_out[...] = (over_rows(grows[0], du[0]) + over_rows(grows[1], du[1])).astype(BF)
    down_out[...] = (over_rows(hid[0], ggrads[0]) + over_rows(hid[1], ggrads[1])).astype(BF)

    @pl.loop(1, NZ)
    def _(step):
        gz_arrival(step).wait_recv()

    def gx_copy(step):
        tiles = gain_out.at[:, x, c]
        return rdma(tiles, tiles, gx_send.at[step], gx_recv.at[step], (z, lax.rem(x + step, NX), c, y))

    def gx_arrival(step):
        source = lax.rem(x + NX - step, NX)
        tiles = gain_out.at[:, source, c]
        return rdma(tiles, tiles, gx_send.at[step], gx_recv.at[step], (z, source, c, y))

    for step in range(1, NX):
        gx_copy(step).start()

    def gc_copy(core):
        tiles = gain_out.at[:, :, core]
        return rdma(tiles, tiles, gc_send.at[0], gc_recv.at[0], partner)

    for k in Z_ORDER:
        if k == 0:

            @pl.when(c == 0)
            def _():
                r_z_home[0].wait()
                r_z_home[1].wait()

            @pl.when(c == 1)
            def _():
                r_z_copy(0).wait()
                r_za_copy(0).wait()
        else:
            r_z_copy(k).wait()
            r_za_copy(k).wait()
    permuted(perm_ref, back_in, sorted_back)
    for q in range(NQ):
        aux_t[q] = aux_z[:, q, :]

    def r_x_copy(step):
        other = lax.rem(me_q + step, NQ)
        return rdma(sorted_back.at[other], out_ref.at[me_q], rx_send.at[step], rx_recv.at[step],
                    (z, lax.rem(other, NX), other // NX, y))

    def r_xa_copy(step):
        other = lax.rem(me_q + step, NQ)
        return rdma(aux_t.at[other], aux_out.at[me_q], rxa_send.at[step], rxa_recv.at[step],
                    (z, lax.rem(other, NX), other // NX, y))

    def r_x_arrival(step):
        source = lax.rem(me_q + NQ - step, NQ)
        device = (z, lax.rem(source, NX), source // NX, y)
        return (
            rdma(sorted_back.at[source], out_ref.at[source], rx_send.at[step], rx_recv.at[step], device),
            rdma(aux_t.at[source], aux_out.at[source], rxa_send.at[step], rxa_recv.at[step], device),
        )

    for step in range(1, NQ):
        r_x_copy(step).start()
        r_xa_copy(step).start()
    out_ref[me_q] = sorted_back[me_q]
    aux_out[me_q] = aux_t[me_q]

    for step in range(1, NX):
        gx_arrival(step).wait_recv()
    gc_copy(c).start()
    gc_copy(1 - c).wait_recv()
    for step in range(1, NQ):
        for arrival in r_x_arrival(step):
            arrival.wait_recv()
    for step in range(1, NQ):
        r_x_copy(step).wait_send()
        r_xa_copy(step).wait_send()
    p_copy().wait_send()
    pa_copy().wait_send()
    gc_copy(c).wait_send()
    for step in range(1, NX):
        gx_copy(step).wait_send()
    for step in range(1, NY):
        gy_copy(step).wait_send()

    @pl.loop(1, NZ)
    def _(step):
        gz_copy(step).wait_send()

    for a in range(2):
        for step in range(1, NQ):
            x_copy(a, step).wait_send()
    for step in range(1, NY):
        g_copy(step).wait_send()

    @pl.loop(1, NZ)
    def _(step):
        dz_copy(step).wait_send()

    for step in range(1, NX):
        dx_copy(step).wait_send()
    dc_copy(c).wait_send()
    for a, k in order:
        if k == 0:

            @pl.when(c == 1)
            def _():
                z_copy(a, 0).wait_send()
        else:
            z_copy(a, k).wait_send()
        y_copy(a, k, True).wait_send()
        y_copy(a, k, False).wait_send()
        f_copy(a, k).wait_send()
        c_copy(a, k).wait_send()
    mc_copy().wait_send()
    for step in range(1, NX):
        mx_copy(step).wait_send()


VMEM_SPEC = pl.BlockSpec(memory_space=pltpu.VMEM)
HBM_SPEC = pl.BlockSpec(memory_space=pl.ANY)
DMA = pltpu.SemaphoreType.DMA


def layer(select, select_weighted, tokens, cotangent, wt, perm, pick, lane, gate, up, down):
    width = tokens.shape[1]
    half = HK // 2
    own = wt.shape[0]
    vm = pltpu.VMEM
    shape = jax.ShapeDtypeStruct
    return pl.pallas_call(
        layer_kernel,
        out_shape=(
            shape((NQ, BLK, width), BF),
            shape((NQ, HK, 128), F32),
            shape((own, width), F32),
            shape((NZ, NX, NC, own, 128), F32),
            shape((tokens.shape[0], NY * width), BF),
            shape((NZ, NX, NC) + wt.shape, BF),
            shape(gate.shape, BF),
            shape(up.shape, BF),
            shape(down.shape, BF),
        ),
        in_specs=[VMEM_SPEC] * 8 + [HBM_SPEC] * 3,
        out_specs=(VMEM_SPEC,) * 9,
        scratch_shapes=[
            vm((NQ, BLK, width), BF),
            vm((NQ, BLK, width), BF),
            vm((NQ, BLK, width), BF),
            vm((NQ, BLK, width), BF),
            vm((NQ, BLK, width), BF),
            vm((NQ, BLK, width), BF),
            vm((NZ, BLK, NY * width), BF),
            vm((NZ, BLK, NY * width), BF),
            vm(gate.shape, BF),
            vm(gate.shape, BF),
            vm(down.shape, BF),
            vm((2, HALF, gate.shape[1]), BF),
            vm((2, HALF, gate.shape[1]), BF),
            vm((2, HALF, gate.shape[1]), BF),
            vm((2, HK, BLK, NY * width), BF),
            vm((HK, BLK, NY * width), BF),
            vm((2, HK, NQ, 128), F32),
            vm((HK, NQ, 128), F32),
            vm((2, NY, half, BLK, width), BF),
            vm((2, 2, half, BLK, width), BF),
            vm((2, half, BLK, width), BF),
            vm((HK, BLK, width), BF),
            vm((HK, BLK, width), BF),
            vm((NQ, BLK, width), BF),
            vm((HK, NQ, 128), F32),
            vm((NY, HK, NQ, 128), F32),
            vm((HK, NQ, 128), F32),
            vm((NQ, HK, 128), F32),
            vm((NZ, NX, NC, own, width), F32),
            vm((NZ, NX, own, width), F32),
            vm((NZ, NX, own, width), F32),
            vm((NX - 1, NZ, own, width), F32),
            vm((NZ, own, width), F32),
            vm((NZ, own, width), F32),
            vm((own, 128), F32),
            vm((own, 128), F32),
            vm((NY, own, 128), F32),
            DMA((9,)),
            DMA((2, NQ)),
            DMA((2, NQ)),
            DMA((2, HK)),
            DMA((2, HK)),
            DMA((2, HK)),
            DMA((2, HK)),
            DMA((2, HK)),
            DMA((2, HK)),
            DMA((2, HK)),
            DMA((2, HK)),
            DMA((2, HK)),
            DMA((2, HK)),
            DMA((NY,)),
            DMA((NY,)),
            DMA((NZ,)),
            DMA((NZ,)),
            DMA((NX,)),
            DMA((NX,)),
            DMA((1,)),
            DMA((1,)),
            DMA((1,)),
            DMA((1,)),
            DMA((NX,)),
            DMA((NX,)),
            DMA((NZ,)),
            DMA((NZ,)),
            DMA((2,)),
            DMA((2,)),
            DMA((2,)),
            DMA((2,)),
            DMA((2,)),
            DMA((2,)),
            DMA((NY,)),
            DMA((NY,)),
            DMA((HK,)),
            DMA((HK,)),
            DMA((HK,)),
            DMA((HK,)),
            DMA((NQ,)),
            DMA((NQ,)),
            DMA((NQ,)),
            DMA((NQ,)),
            DMA((NY,)),
            DMA((NY,)),
            DMA((NZ,)),
            DMA((NZ,)),
            DMA((NX,)),
            DMA((NX,)),
            DMA((1,)),
            DMA((1,)),
        ],
        compiler_params=pltpu.CompilerParams(
            collective_id=0, has_side_effects=True, vmem_limit_bytes=60 * 1024 * 1024
        ),
        name="layer",
    )(select, select_weighted, tokens, cotangent, wt, perm, pick, lane, gate, up, down)


def local(tokens, cotangent, routes, route_weights, w_gate, w_up, w_down, dense_weight, mix_gate):
    z, x, c = (lax.axis_index(a) for a in EP)
    token_count = routes.shape[0]
    ep_count = NZ * NX * NC
    e = jnp.arange(EXPERTS, dtype=jnp.int32)
    expert = lax.rem(z + 2 * lax.rem(e, HK) + e // (HK * NX), NZ) * NX + lax.rem(e // HK, NX)
    picked = routes.T
    hits = [picked[p][None, :] == expert[:, None] for p in range(2)]
    hit = hits[0] | hits[1]
    t = jnp.arange(token_count, dtype=jnp.int32)
    earlier = (t[:, None] < t[None, :]).astype(BF)
    rank = jnp.dot(hit.astype(BF), earlier, preferred_element_type=F32).astype(jnp.int32)
    s = jnp.arange(CAP, dtype=jnp.int32)
    chosen = (hit[:, None, :] & (rank[:, None, :] == s[None, :, None])).reshape(-1, token_count)
    weights = route_weights.T
    weight = jnp.where(hits[0], weights[0][None, :], weights[1][None, :])
    weight = jnp.broadcast_to(weight[:, None, :], (EXPERTS, CAP, token_count)).reshape(-1, token_count)
    select = chosen.astype(BF)
    select_weighted = jnp.where(chosen, weight, jnp.zeros_like(weight))
    r = jnp.arange(NQ * BLK, dtype=jnp.int32)
    moved = lax.rem(r, BLK) // CAP * BLK + r // BLK * CAP + lax.rem(r, CAP)
    perm = (moved[:, None] == r[None, :]).astype(BF)
    groups = jnp.arange(HK * NQ, dtype=jnp.int32)
    pick = (r[None, :] // CAP == groups[:, None]).astype(BF)
    lane = (lax.rem(r, CAP)[:, None] == jnp.arange(128, dtype=jnp.int32)[None, :]).astype(F32)
    slots, aux_back, moment_own, gain_all, cot_full, wt_full, gate_grad, up_grad, down_grad = layer(
        select, select_weighted, tokens, cotangent, dense_weight.T, perm, pick, lane,
        w_gate[0], w_up[0], w_down[0],
    )
    own = dense_weight.shape[1]
    wt_full = wt_full.reshape(ep_count * own, -1)
    scaled = (mix_gate[None, :] * cot_full.astype(F32)).astype(BF)
    dense_dx = jnp.dot(scaled, wt_full, preferred_element_type=F32)
    token_grad = (dense_dx + dot(select, slots.reshape(NQ * BLK, -1), ROWS_BY)).astype(BF)
    values = aux_back[:, :, :CAP].reshape(EXPERTS, CAP)
    at_slot = jnp.sum(
        jnp.where(rank[:, :, None] == s[None, None, :], values[:, None, :], 0.0), axis=2
    )
    route_sums = jnp.stack([jnp.sum(jnp.where(h, at_slot, 0.0), axis=0) for h in hits], axis=1)
    route_grad = route_sums / route_weights.astype(F32)
    ep_index = (z * NX + x) * NC + c
    own_gate = lax.dynamic_slice(mix_gate, (ep_index * own,), (own,))
    dense_grad = (moment_own * (own_gate[:, None] * (1.0 / ep_count))).T
    mix_grad = gain_all[..., 0].reshape(-1) / ep_count
    return token_grad, route_grad, gate_grad[None], up_grad[None], down_grad[None], dense_grad, mix_grad


def solution(mesh):
    finer = Mesh(mesh.devices.reshape(NZ, NX, NC, NY), EP + ("y",))
    in_specs = (
        P(EP, "y"),
        P(EP, "y"),
        P(EP, None),
        P(EP, None),
        P(EP, None, "y"),
        P(EP, None, "y"),
        P(EP, "y", None),
        P("y", EP),
        P(),
    )
    out_specs = (
        P(EP, "y"),
        P(EP, None),
        P(EP, None, "y"),
        P(EP, None, "y"),
        P(EP, "y", None),
        P("y", EP),
        P(),
    )
    return jax.shard_map(local, mesh=finer, in_specs=in_specs, out_specs=out_specs, check_vma=False)
```

```python
import functools

import jax
import jax.numpy as jnp
from jax import lax
from jax.experimental import pallas as pl
from jax.experimental.pallas import tpu as pltpu
from jax.sharding import Mesh
from jax.sharding import PartitionSpec as P

EP = ("z", "x", "c")
MESH = pl.DeviceIdType.MESH
BF = jnp.bfloat16
F32 = jnp.float32
NZ = 16
NX = 4
NC = 2
NY = 4
CAP = 5
HK = NZ // NC
NQ = NX * NC
BLK = NQ * CAP
Z_ORDER = (0, 1, 7, 2, 6, 3, 5, 4)


def rdma(src, dst, send, recv, device):
    return pltpu.make_async_remote_copy(
        src_ref=src, dst_ref=dst, send_sem=send, recv_sem=recv, device_id=device, device_id_type=MESH
    )


def where_am_i():
    return tuple(lax.axis_index(a) for a in ("z", "x", "c", "y"))


def greet_all():
    z, x, c, y = where_am_i()
    barrier = pltpu.get_barrier_semaphore()

    def greet(device):
        pl.semaphore_signal(barrier, inc=1, device_id=device, device_id_type=MESH)

    for step in range(1, NQ):
        other = lax.rem(c * NX + x + step, NQ)
        greet((z, lax.rem(other, NX), other // NX, y))
    for step in range(1, NZ):
        greet((lax.rem(z + step, NZ), x, c, y))
    for step in range(1, NY):
        greet((z, x, c, lax.rem(y + step, NY)))


def wait_all():
    pl.semaphore_wait(pltpu.get_barrier_semaphore(), NQ - 1 + NZ - 1 + NY - 1)


def cols(index, width):
    return pl.ds(pl.multiple_of(index * width, width), width)


def permuted(perm_ref, value_ref, out_ref):
    width = value_ref.shape[-1]
    flat = value_ref[...].reshape(NQ * BLK, width)
    moved = jnp.dot(perm_ref[...], flat, preferred_element_type=F32).astype(BF)
    out_ref[...] = moved.reshape(NQ, BLK, width)


HALF = HK * BLK
LAG_F = 3
LAG_C = 6
PLAIN = (((1,), (0,)), ((), ()))
ROWS_BY = (((0,), (0,)), ((), ()))
COLS_BY = (((1,), (1,)), ((), ()))


def dot(a, b, dims):
    return lax.dot_general(a, b, dims, preferred_element_type=F32)


def gathered_rows(select, value_ref):
    rows = dot(select, value_ref[...], PLAIN).astype(BF)
    return rows.reshape(NQ, BLK, value_ref.shape[1])


def over_40(value):
    return (value * 52429) >> 21


def over_5(value):
    return (value * 52429) >> 18


def iota(shape, dim):
    return lax.broadcasted_iota(jnp.int32, shape, dim)


def ones_where(mask, dtype):
    return jnp.where(mask, 1.0, 0.0).astype(dtype)


def exact_dot(one_hot, value):
    high = value.astype(BF)
    low = (value - high.astype(F32)).astype(BF)
    return dot(one_hot, high, PLAIN) + dot(one_hot, low, PLAIN)


def layer_kernel(
    tokens_ref, cot_ref, routes_ref, weights_ref, wt_ref, mix_ref,
    wg_hbm, wu_hbm, wd_hbm,
    token_out, route_out, gate_out, up_out, down_out, dense_out, mix_out,
    *scratch,
):
    (
        s_tok, s_cot, x_tok, x_cot, p_tok, p_cot, rows_ref, grads_ref, wg, wu, wd, hid, dg, du,
        part, p_in, aux, aux_in, first, first_in, second_in, back, back_in, sorted_back, aux_sum,
        aux_y, aux_z, aux_t, moment_ref, m_in, m_half, m_x, m_xsum, m_z, g_mine, g_own, g_y,
        local_sem, x_send, x_recv, z_send, z_recv, yp_send, yp_recv, ym_send, ym_recv, f_send,
        f_recv, c_send, c_recv, g_send, g_recv, dz_send, dz_recv, dx_send, dx_recv, dc_send,
        dc_recv, mc_send, mc_recv, mx_send, mx_recv, mz_send, mz_recv, p_send, p_recv, b1_send,
        b1_recv, b2_send, b2_recv, ay_send, ay_recv, rz_send, rz_recv, rza_send, rza_recv, rx_send,
        rx_recv, rxa_send, rxa_recv, gy_send, gy_recv, gz_send, gz_recv, gx_send, gx_recv, gc_send,
        gc_recv,
        perm_ref, sel_ref, chosen_ref, full_ref, dense_ref, out_ref, aux_out, az_out, gain_out, pg, pu, dx_acc,
        gate_s, up_s, down_s, put_sem,
    ) = scratch
    z, x, c, y = where_am_i()
    width = tokens_ref.shape[-1]
    me_q = c * NX + x
    y_up, y_down = lax.rem(y + 1, NY), lax.rem(y + NY - 1, NY)
    y_far = lax.rem(y + 2, NY)
    partner = (z, x, 1 - c, y)
    slots = (s_tok, s_cot)
    gathered = (x_tok, x_cot)
    sorted_rows = (p_tok, p_cot)
    outs = (rows_ref, grads_ref)

    own = [
        pltpu.make_async_copy(cot_ref, full_ref.at[:, cols(y, width)], local_sem.at[0]),
        pltpu.make_async_copy(wt_ref, dense_ref.at[z, x, c], local_sem.at[1]),
    ]
    for copy in own:
        copy.start()
    weights = [
        pltpu.make_async_copy(wg_hbm, wg, local_sem.at[6]),
        pltpu.make_async_copy(wu_hbm, wu, local_sem.at[7]),
        pltpu.make_async_copy(wd_hbm, wd, local_sem.at[8]),
    ]
    for copy in weights:
        copy.start()
    greet_all()
    table = (NQ * BLK, tokens_ref.shape[0])
    row = iota(table, 0)
    line = over_40(row)
    rest = row - BLK * line
    step_k = over_5(rest)
    slot = rest - CAP * step_k
    expert = ((z + 2 * step_k + (line >> 2)) & (NZ - 1)) * NX + (line & (NX - 1))
    hit_first = routes_ref[0:1, :] == expert
    hit_second = routes_ref[1:2, :] == expert
    square = (table[1], table[1])
    earlier = ones_where(iota(square, 0) < iota(square, 1), BF)
    hit = ones_where(hit_first, F32) + ones_where(hit_second, F32)
    rank = dot(hit.astype(BF), earlier, PLAIN)
    at_slot = ones_where(rank == slot.astype(F32), F32)
    chosen_ref[0] = ones_where(hit_first, F32) * at_slot
    chosen_ref[1] = ones_where(hit_second, F32) * at_slot
    gate_weights = weights_ref[...].astype(F32)
    select = (hit * at_slot).astype(BF)
    sel_ref[...] = select
    select_weighted = (chosen_ref[0] * gate_weights[0:1, :] + chosen_ref[1] * gate_weights[1:2, :]).astype(BF)
    slots[0][...] = gathered_rows(select, tokens_ref)
    slots[1][...] = gathered_rows(select_weighted, cot_ref)
    both_ways = (NQ * BLK, NQ * BLK)
    place = iota(both_ways, 0)
    block = over_40(place)
    inside = place - BLK * block
    source = over_5(inside)
    perm_ref[...] = ones_where(
        source * BLK + block * CAP + (inside - CAP * source) == iota(both_ways, 1), BF
    )
    wait_all()

    def x_copy(a, step):
        other = lax.rem(me_q + step, NQ)
        return rdma(
            slots[a].at[other], gathered[a].at[me_q], x_send.at[a, step], x_recv.at[a, step],
            (z, lax.rem(other, NX), other // NX, y),
        )

    def x_arrival(a, step):
        source = lax.rem(me_q + NQ - step, NQ)
        return rdma(
            slots[a].at[source], gathered[a].at[source], x_send.at[a, step], x_recv.at[a, step],
            (z, lax.rem(source, NX), source // NX, y),
        )

    for a in range(2):
        for step in range(1, NQ):
            x_copy(a, step).start()

    def g_copy(step):
        return rdma(
            cot_ref, full_ref.at[:, cols(y, width)], g_send.at[step], g_recv.at[step],
            (z, x, c, lax.rem(y + step, NY)),
        )

    def g_arrival(step):
        source = lax.rem(y + NY - step, NY)
        return rdma(
            cot_ref, full_ref.at[:, cols(source, width)], g_send.at[step], g_recv.at[step],
            (z, x, c, source),
        )

    for step in range(1, NY):
        g_copy(step).start()

    def dz_copy(step):
        return rdma(
            wt_ref, dense_ref.at[z, x, c], dz_send.at[step], dz_recv.at[step],
            (lax.rem(z + step, NZ), x, c, y),
        )

    def dz_arrival(step):
        source = lax.rem(z + NZ - step, NZ)
        return rdma(
            wt_ref, dense_ref.at[source, x, c], dz_send.at[step], dz_recv.at[step], (source, x, c, y)
        )

    @pl.loop(1, NZ)
    def _(step):
        dz_copy(step).start()

    def z_copy(a, k):
        target = lax.rem(z + 2 * k + c, NZ)
        return rdma(
            sorted_rows[a].at[k], outs[a].at[c * HK + k, :, cols(y, width)],
            z_send.at[a, k], z_recv.at[a, k], (target, x, c, y),
        )

    def z_home(a):
        return pltpu.make_async_copy(
            sorted_rows[a].at[0], outs[a].at[0, :, cols(y, width)], local_sem.at[2 + a]
        )

    for a in range(2):
        gathered[a][me_q] = slots[a][me_q]
        for step in range(1, NQ):
            x_arrival(a, step).wait_recv()
        permuted(perm_ref, gathered[a], sorted_rows[a])
        for k in Z_ORDER:
            if k == 0:

                @pl.when(c == 0)
                def _():
                    z_home(a).start()

                @pl.when(c == 1)
                def _():
                    z_copy(a, 0).start()
            else:
                z_copy(a, k).start()

    def y_copy(a, k, up):
        part = outs[a].at[c * HK + k, :, cols(y, width)]
        if up:
            return rdma(part, part, yp_send.at[a, k], yp_recv.at[a, k], (z, x, c, y_up))
        return rdma(part, part, ym_send.at[a, k], ym_recv.at[a, k], (z, x, c, y_down))

    def y_arrival(a, k, up):
        if up:
            part = outs[a].at[c * HK + k, :, cols(y_down, width)]
            return rdma(part, part, yp_send.at[a, k], yp_recv.at[a, k], (z, x, c, y_down))
        part = outs[a].at[c * HK + k, :, cols(y_up, width)]
        return rdma(part, part, ym_send.at[a, k], ym_recv.at[a, k], (z, x, c, y_up))

    def f_copy(a, k):
        source, target = (y_down, y_up) if k % 2 == 0 else (y_up, y_down)
        part = outs[a].at[c * HK + k, :, cols(source, width)]
        return rdma(part, part, f_send.at[a, k], f_recv.at[a, k], (z, x, c, target))

    def f_arrival(a, k):
        part = outs[a].at[c * HK + k, :, cols(y_far, width)]
        return rdma(part, part, f_send.at[a, k], f_recv.at[a, k], (z, x, c, y_up))

    def c_copy(a, k):
        block = outs[a].at[c * HK + k]
        return rdma(block, block, c_send.at[a, k], c_recv.at[a, k], partner)

    def c_arrival(a, k):
        block = outs[a].at[(1 - c) * HK + k]
        return rdma(block, block, c_send.at[a, k], c_recv.at[a, k], partner)

    def dx_copy(step):
        part = dense_ref.at[:, x, c]
        return rdma(part, part, dx_send.at[step], dx_recv.at[step], (z, lax.rem(x + step, NX), c, y))

    def dx_arrival(step):
        source = lax.rem(x + NX - step, NX)
        part = dense_ref.at[:, source, c]
        return rdma(part, part, dx_send.at[step], dx_recv.at[step], (z, source, c, y))

    def dc_copy(core):
        part = dense_ref.at[:, :, core]
        return rdma(part, part, dc_send.at[0], dc_recv.at[0], partner)

    own[0].wait()
    for step in range(1, NY):
        g_arrival(step).wait_recv()
    moment_ref[...] = dot(full_ref[...], tokens_ref[...], ROWS_BY).reshape(moment_ref.shape)

    def mc_copy():
        return rdma(moment_ref.at[:, :, 1 - c], m_in, mc_send.at[0], mc_recv.at[0], partner)

    mc_copy().start()

    def mx_copy(step):
        other = lax.rem(x + step, NX)
        return rdma(m_half.at[:, other], m_x.at[step - 1], mx_send.at[step], mx_recv.at[step],
                    (z, other, c, y))

    def mz_copy(step):
        other = lax.rem(z + step, NZ)
        return rdma(m_xsum.at[other], m_z.at[step], mz_send.at[step], mz_recv.at[step],
                    (other, x, c, y))

    def rows_of(ref, turn):
        group = jnp.where(turn == 0, 1 - c, c)
        return ref[pl.ds(group * HK, HK)].reshape(HALF, NY * width)

    order = [(a, k) for a in range(2) for k in Z_ORDER]
    for i in range(len(order) + LAG_C):
        if i < len(order):
            a, k = order[i]
            if k == 0:

                @pl.when(c == 0)
                def _():
                    z_home(a).wait()

                @pl.when(c == 1)
                def _():
                    z_copy(a, 0).wait_recv()
            else:
                z_copy(a, k).wait_recv()
            y_copy(a, k, True).start()
            y_copy(a, k, False).start()
        if LAG_F <= i < len(order) + LAG_F:
            a, k = order[i - LAG_F]
            up = k % 2 == 0
            y_arrival(a, k, up).wait_recv()
            f_copy(a, k).start()
            y_arrival(a, k, not up).wait_recv()
        if i >= LAG_C:
            a, k = order[i - LAG_C]
            f_arrival(a, k).wait_recv()
            c_copy(a, k).start()
        if i == 6:
            own[1].wait()

            @pl.loop(1, NZ)
            def _(step):
                dz_arrival(step).wait_recv()

            for step in range(1, NX):
                dx_copy(step).start()
        if i == 8:
            mc_copy().wait_recv()
            for n in range(NX):
                m_half[:, n] = moment_ref[:, n, c] + m_in[:, n]
            for step in range(1, NX):
                mx_copy(step).start()
        if i == 13:
            for copy in weights:
                copy.wait()
            for k in Z_ORDER:
                c_arrival(0, k).wait_recv()
        if 14 <= i < 18:
            turn = (i - 14) // 2
            if i % 2 == 0:
                pg[turn] = dot(rows_of(rows_ref, turn), wg[...], COLS_BY)
            else:
                pu[turn] = dot(rows_of(rows_ref, turn), wu[...], COLS_BY)
        if i == 20:
            for step in range(1, NX):
                mx_copy(step).wait_recv()
            m_xsum[...] = m_half[:, x] + m_x[0] + m_x[1] + m_x[2]

            @pl.loop(1, NZ)
            def _(step):
                mz_copy(step).start()
        if i == 12:
            for step in range(1, NX):
                dx_arrival(step).wait_recv()
            dc_copy(c).start()

    dc_copy(1 - c).wait_recv()
    for k in Z_ORDER:
        c_arrival(1, k).wait_recv()

    def p_copy():
        return rdma(part.at[0], p_in, p_send.at[0], p_recv.at[0], partner)

    def pa_copy():
        return rdma(aux.at[0], aux_in, p_send.at[1], p_recv.at[1], partner)

    @pl.loop(0, 2)
    def _(turn):
        pre_gate = pg[turn]
        pre_up = pu[turn]
        back_h = dot(rows_of(grads_ref, turn), wd[...], COLS_BY)
        sig = jax.nn.sigmoid(pre_gate)
        act = pre_gate * sig
        hidden_bf = (act * pre_up).astype(BF)
        hid[turn] = hidden_bf
        d_gate = (back_h * pre_up * sig * (1.0 + pre_gate * (1.0 - sig))).astype(BF)
        d_up = (back_h * act).astype(BF)
        dg[turn] = d_gate
        du[turn] = d_up
        route = jnp.sum(hidden_bf.astype(F32) * back_h, axis=1, keepdims=True)
        at = (HALF, 128)
        lane_is = over_40(iota(at, 0)) * -BLK + iota(at, 0) == iota(at, 1)
        block_of = ones_where(over_40(iota((HK, HALF), 1)) == iota((HK, HALF), 0), BF)
        aux[turn] = exact_dot(block_of, jnp.where(lane_is, route, 0.0))
        both_parts = dot(d_gate, wg[...], PLAIN) + dot(d_up, wu[...], PLAIN)
        part[turn] = both_parts.astype(BF).reshape(HK, BLK, NY * width)

        @pl.when(turn == 0)
        def _():
            p_copy().start()
            pa_copy().start()

    half = HK // 2
    flip1 = y + 1 - 2 * lax.rem(y, 2)
    flip3 = NY - 1 - y
    flip2 = lax.rem(y + 2, NY)
    pairs = ((flip1, flip3), (flip3, flip1))

    p_copy().wait_recv()

    def b1_copy(h):
        return rdma(
            first.at[h, pl.ds(2, 2)], first_in.at[h], b1_send.at[h], b1_recv.at[h],
            (z, x, c, pairs[h][0]),
        )

    def both(h, i, owner):
        for j in range(half):
            mine = part[1, h * half + j, :, cols(owner, width)].astype(F32)
            theirs = p_in[h * half + j, :, cols(owner, width)].astype(F32)
            first[h, i, j] = (mine + theirs).astype(BF)

    for h in range(2):
        both(h, 2, pairs[h][0])
        both(h, 3, flip2)
        b1_copy(h).start()
    for h in range(2):
        both(h, 0, y)
        both(h, 1, pairs[h][1])

    pa_copy().wait_recv()
    aux_sum[...] = aux[1] + aux_in[...]

    def ay_copy(step):
        return rdma(aux_sum, aux_y.at[y], ay_send.at[step], ay_recv.at[step],
                    (z, x, c, lax.rem(y + step, NY)))

    def ay_arrival(step):
        source = lax.rem(y + NY - step, NY)
        return rdma(aux_sum, aux_y.at[source], ay_send.at[step], ay_recv.at[step], (z, x, c, source))

    for step in range(1, NY):
        ay_copy(step).start()
    aux_y[y] = aux_sum[...]

    def b2_copy(h):
        return rdma(first.at[h, 3], second_in.at[h], b2_send.at[h], b2_recv.at[h],
                    (z, x, c, pairs[h][1]))

    for h in range(2):
        b1_copy(h).wait()
        first[h, 3] = (first[h, 1].astype(F32) + first_in[h, 1].astype(F32)).astype(BF)
        b2_copy(h).start()

    for step in range(1, NY):
        ay_arrival(step).wait_recv()
        ay_copy(step).wait_send()
    aux_sum[...] = aux_y[0] + aux_y[1] + aux_y[2] + aux_y[3]
    for k in range(HK):
        az_out[k] = aux_sum[k : k + 1]

    def r_z_copy(k):
        target = lax.rem(z + 2 * NZ - 2 * k - c, NZ)
        return rdma(back.at[k], back_in.at[k], rz_send.at[k], rz_recv.at[k], (target, x, c, y))

    def r_za_copy(k):
        target = lax.rem(z + 2 * NZ - 2 * k - c, NZ)
        return rdma(az_out.at[k], aux_z.at[k], rza_send.at[k], rza_recv.at[k], (target, x, c, y))

    r_z_home = [
        pltpu.make_async_copy(back.at[0], back_in.at[0], local_sem.at[4]),
        pltpu.make_async_copy(az_out.at[0], aux_z.at[0], local_sem.at[5]),
    ]

    def send_back(k):
        if k == 0:

            @pl.when(c == 0)
            def _():
                r_z_home[0].start()
                r_z_home[1].start()

            @pl.when(c == 1)
            def _():
                r_z_copy(0).start()
                r_za_copy(0).start()
        else:
            r_z_copy(k).start()
            r_za_copy(k).start()

    for h in range(2):
        b2_copy(h).wait()
        back[pl.ds(h * half, half)] = (
            first[h, 0].astype(F32) + first_in[h, 0].astype(F32) + second_in[h].astype(F32)
        ).astype(BF)
    for k in Z_ORDER:
        send_back(k)

    m_z[0] = m_xsum[z]

    @pl.loop(1, NZ)
    def _(step):
        mz_copy(step).wait()

    moment_own = jnp.sum(m_z[...], axis=0)
    ep_index = (z * NX + x) * NC + c
    here = (moment_own.shape[0], NY * width)
    is_own = iota(here, 1) == ep_index * here[0] + iota(here, 0)
    own_gate = jnp.sum(jnp.where(is_own, mix_ref[...], 0.0), axis=1, keepdims=True)
    dense_out[...] = moment_own * (own_gate * (1.0 / (NZ * NX * NC)))
    gain = jnp.sum(wt_ref[...].astype(F32) * moment_own, axis=1, keepdims=True)
    g_mine[...] = jnp.broadcast_to(gain, g_mine.shape)

    def gy_copy(step):
        return rdma(g_mine, g_y.at[y], gy_send.at[step], gy_recv.at[step],
                    (z, x, c, lax.rem(y + step, NY)))

    def gy_arrival(step):
        source = lax.rem(y + NY - step, NY)
        return rdma(g_mine, g_y.at[source], gy_send.at[step], gy_recv.at[step], (z, x, c, source))

    for step in range(1, NY):
        gy_copy(step).start()
    g_y[y] = g_mine[...]

    puts = [
        pltpu.make_async_copy(source, target, put_sem.at[i])
        for i, (source, target) in enumerate(((gate_s, gate_out), (up_s, up_out), (down_s, down_out)))
    ]

    def over_rows(a, b):
        return dot(a, b, ROWS_BY)

    down_s[...] = (
        over_rows(hid[0], rows_of(grads_ref, 0)) + over_rows(hid[1], rows_of(grads_ref, 1))
    ).astype(BF)
    puts[2].start()
    for step in range(1, NY):
        gy_arrival(step).wait_recv()
    g_own[...] = g_y[0] + g_y[1] + g_y[2] + g_y[3]

    def gz_copy(step):
        return rdma(g_own, gain_out.at[z, x, c], gz_send.at[step], gz_recv.at[step],
                    (lax.rem(z + step, NZ), x, c, y))

    def gz_arrival(step):
        source = lax.rem(z + NZ - step, NZ)
        return rdma(g_own, gain_out.at[source, x, c], gz_send.at[step], gz_recv.at[step],
                    (source, x, c, y))

    @pl.loop(1, NZ)
    def _(step):
        gz_copy(step).start()

    gain_out[z, x, c] = g_own[...]

    gate_s[...] = (
        over_rows(dg[0], rows_of(rows_ref, 0)) + over_rows(dg[1], rows_of(rows_ref, 1))
    ).astype(BF)
    puts[0].start()
    up_s[...] = (
        over_rows(du[0], rows_of(rows_ref, 0)) + over_rows(du[1], rows_of(rows_ref, 1))
    ).astype(BF)
    puts[1].start()
    scaled = (mix_ref[...] * full_ref[...].astype(F32)).astype(BF)
    dx_acc[...] = dot(scaled, dense_ref[...].reshape(NY * width, width), PLAIN)

    @pl.loop(1, NZ)
    def _(step):
        gz_arrival(step).wait_recv()

    def gx_copy(step):
        tiles = gain_out.at[:, x, c]
        return rdma(tiles, tiles, gx_send.at[step], gx_recv.at[step], (z, lax.rem(x + step, NX), c, y))

    def gx_arrival(step):
        source = lax.rem(x + NX - step, NX)
        tiles = gain_out.at[:, source, c]
        return rdma(tiles, tiles, gx_send.at[step], gx_recv.at[step], (z, source, c, y))

    for step in range(1, NX):
        gx_copy(step).start()

    def gc_copy(core):
        tiles = gain_out.at[:, :, core]
        return rdma(tiles, tiles, gc_send.at[0], gc_recv.at[0], partner)

    for k in Z_ORDER:
        if k == 0:

            @pl.when(c == 0)
            def _():
                r_z_home[0].wait()
                r_z_home[1].wait()

            @pl.when(c == 1)
            def _():
                r_z_copy(0).wait()
                r_za_copy(0).wait()
        else:
            r_z_copy(k).wait()
            r_za_copy(k).wait()
    permuted(perm_ref, back_in, sorted_back)
    for k in range(HK):
        aux_t[k : k + 1] = aux_z[k]

    def r_x_copy(step):
        other = lax.rem(me_q + step, NQ)
        return rdma(sorted_back.at[other], out_ref.at[me_q], rx_send.at[step], rx_recv.at[step],
                    (z, lax.rem(other, NX), other // NX, y))

    def r_xa_copy(step):
        other = lax.rem(me_q + step, NQ)
        return rdma(aux_t, aux_out.at[me_q], rxa_send.at[step], rxa_recv.at[step],
                    (z, lax.rem(other, NX), other // NX, y))

    def r_x_arrival(step):
        source = lax.rem(me_q + NQ - step, NQ)
        device = (z, lax.rem(source, NX), source // NX, y)
        return (
            rdma(sorted_back.at[source], out_ref.at[source], rx_send.at[step], rx_recv.at[step], device),
            rdma(aux_t, aux_out.at[source], rxa_send.at[step], rxa_recv.at[step], device),
        )

    for step in range(1, NQ):
        r_x_copy(step).start()
        r_xa_copy(step).start()
    out_ref[me_q] = sorted_back[me_q]
    aux_out[me_q] = aux_t[...]

    for step in range(1, NX):
        gx_arrival(step).wait_recv()
    gc_copy(c).start()
    gc_copy(1 - c).wait_recv()
    for step in range(1, NQ):
        for arrival in r_x_arrival(step):
            arrival.wait_recv()
    token_out[...] = (
        dx_acc[...] + dot(sel_ref[...], out_ref[...].reshape(NQ * BLK, width), ROWS_BY)
    ).astype(BF)
    group_of = ones_where(over_5(iota((NQ * BLK, HK * NQ), 0)) == iota((NQ * BLK, HK * NQ), 1), BF)
    values = exact_dot(group_of, aux_out[...].reshape(HK * NQ, 128))
    at = (NQ * BLK, 128)
    lane_is = iota(at, 0) - CAP * over_5(iota(at, 0)) + me_q * CAP == iota(at, 1)
    value = jnp.sum(jnp.where(lane_is, values, 0.0), axis=1, keepdims=True)
    home_weights = weights_ref[...].astype(F32)
    for p in range(2):
        total = jnp.sum(chosen_ref[p] * value, axis=0, keepdims=True)
        route_out[p : p + 1, :] = total / home_weights[p : p + 1, :]
    tiles_in = gain_out[...].reshape(NZ * NX * NC * here[0], 128)
    diagonal = ones_where(iota((128, 128), 0) == iota((128, 128), 1), F32)
    for n in range(NZ * NX * NC * here[0] // 128):
        picked = jnp.sum(tiles_in[n * 128 : (n + 1) * 128] * diagonal, axis=0, keepdims=True)
        mix_out[n : n + 1, :] = picked * (1.0 / (NZ * NX * NC))
    for copy in puts:
        copy.wait()
    for step in range(1, NQ):
        r_x_copy(step).wait_send()
        r_xa_copy(step).wait_send()
    p_copy().wait_send()
    pa_copy().wait_send()
    gc_copy(c).wait_send()
    for step in range(1, NX):
        gx_copy(step).wait_send()
    for step in range(1, NY):
        gy_copy(step).wait_send()

    @pl.loop(1, NZ)
    def _(step):
        gz_copy(step).wait_send()

    for a in range(2):
        for step in range(1, NQ):
            x_copy(a, step).wait_send()
    for step in range(1, NY):
        g_copy(step).wait_send()

    @pl.loop(1, NZ)
    def _(step):
        dz_copy(step).wait_send()

    for step in range(1, NX):
        dx_copy(step).wait_send()
    dc_copy(c).wait_send()
    for a, k in order:
        if k == 0:

            @pl.when(c == 1)
            def _():
                z_copy(a, 0).wait_send()
        else:
            z_copy(a, k).wait_send()
        y_copy(a, k, True).wait_send()
        y_copy(a, k, False).wait_send()
        f_copy(a, k).wait_send()
        c_copy(a, k).wait_send()
    mc_copy().wait_send()
    for step in range(1, NX):
        mx_copy(step).wait_send()


VMEM_SPEC = pl.BlockSpec(memory_space=pltpu.VMEM)
HBM_SPEC = pl.BlockSpec(memory_space=pl.ANY)
DMA = pltpu.SemaphoreType.DMA


def layer(tokens, cotangent, routes, weights, wt, mix_gate, gate, up, down):
    width = tokens.shape[1]
    half = HK // 2
    own = wt.shape[0]
    hidden = gate.shape[0]
    vm = pltpu.VMEM
    shape = jax.ShapeDtypeStruct
    return pl.pallas_call(
        layer_kernel,
        out_shape=(
            shape(tokens.shape, BF),
            shape(routes.shape, F32),
            shape(gate.shape, BF),
            shape(up.shape, BF),
            shape(down.shape, BF),
            shape(wt.shape, F32),
            shape((NY * width // 128, 128), F32),
        ),
        in_specs=[VMEM_SPEC] * 6 + [HBM_SPEC] * 3,
        out_specs=(VMEM_SPEC,) * 2 + (HBM_SPEC,) * 3 + (VMEM_SPEC,) * 2,
        scratch_shapes=[
            vm((NQ, BLK, width), BF),
            vm((NQ, BLK, width), BF),
            vm((NQ, BLK, width), BF),
            vm((NQ, BLK, width), BF),
            vm((NQ, BLK, width), BF),
            vm((NQ, BLK, width), BF),
            vm((NZ, BLK, NY * width), BF),
            vm((NZ, BLK, NY * width), BF),
            vm(gate.shape, BF),
            vm(gate.shape, BF),
            vm(down.shape, BF),
            vm((2, HALF, hidden), BF),
            vm((2, HALF, hidden), BF),
            vm((2, HALF, hidden), BF),
            vm((2, HK, BLK, NY * width), BF),
            vm((HK, BLK, NY * width), BF),
            vm((2, HK, 128), F32),
            vm((HK, 128), F32),
            vm((2, NY, half, BLK, width), BF),
            vm((2, 2, half, BLK, width), BF),
            vm((2, half, BLK, width), BF),
            vm((HK, BLK, width), BF),
            vm((HK, BLK, width), BF),
            vm((NQ, BLK, width), BF),
            vm((HK, 128), F32),
            vm((NY, HK, 128), F32),
            vm((HK, 1, 128), F32),
            vm((HK, 128), F32),
            vm((NZ, NX, NC, own, width), F32),
            vm((NZ, NX, own, width), F32),
            vm((NZ, NX, own, width), F32),
            vm((NX - 1, NZ, own, width), F32),
            vm((NZ, own, width), F32),
            vm((NZ, own, width), F32),
            vm((own, 128), F32),
            vm((own, 128), F32),
            vm((NY, own, 128), F32),
            DMA((9,)),
            DMA((2, NQ)),
            DMA((2, NQ)),
            DMA((2, HK)),
            DMA((2, HK)),
            DMA((2, HK)),
            DMA((2, HK)),
            DMA((2, HK)),
            DMA((2, HK)),
            DMA((2, HK)),
            DMA((2, HK)),
            DMA((2, HK)),
            DMA((2, HK)),
            DMA((NY,)),
            DMA((NY,)),
            DMA((NZ,)),
            DMA((NZ,)),
            DMA((NX,)),
            DMA((NX,)),
            DMA((1,)),
            DMA((1,)),
            DMA((1,)),
            DMA((1,)),
            DMA((NX,)),
            DMA((NX,)),
            DMA((NZ,)),
            DMA((NZ,)),
            DMA((2,)),
            DMA((2,)),
            DMA((2,)),
            DMA((2,)),
            DMA((2,)),
            DMA((2,)),
            DMA((NY,)),
            DMA((NY,)),
            DMA((HK,)),
            DMA((HK,)),
            DMA((HK,)),
            DMA((HK,)),
            DMA((NQ,)),
            DMA((NQ,)),
            DMA((NQ,)),
            DMA((NQ,)),
            DMA((NY,)),
            DMA((NY,)),
            DMA((NZ,)),
            DMA((NZ,)),
            DMA((NX,)),
            DMA((NX,)),
            DMA((1,)),
            DMA((1,)),
            vm((NQ * BLK, NQ * BLK), BF),
            vm((NQ * BLK, tokens.shape[0]), BF),
            vm((2, NQ * BLK, tokens.shape[0]), F32),
            vm((tokens.shape[0], NY * width), BF),
            vm((NZ, NX, NC) + wt.shape, BF),
            vm((NQ, BLK, width), BF),
            vm((NQ, HK, 128), F32),
            vm((HK, 1, 128), F32),
            vm((NZ, NX, NC, own, 128), F32),
            vm((2, HALF, hidden), F32),
            vm((2, HALF, hidden), F32),
            vm(tokens.shape, F32),
            vm(gate.shape, BF),
            vm(gate.shape, BF),
            vm(down.shape, BF),
            DMA((3,)),
        ],
        compiler_params=pltpu.CompilerParams(
            collective_id=0, has_side_effects=True, vmem_limit_bytes=60 * 1024 * 1024
        ),
        name="layer",
    )(tokens, cotangent, routes, weights, wt, mix_gate, gate, up, down)


def put_kernel(count, *refs):
    ins, outs, held, sems = refs[:count], refs[count : 2 * count], refs[2 * count : -1], refs[-1]
    first = [pltpu.make_async_copy(ins[i], held[i], sems.at[0, i]) for i in range(count)]
    second = [pltpu.make_async_copy(held[i], outs[i], sems.at[1, i]) for i in range(count)]
    for copy in first:
        copy.start()
    for i in range(count):
        first[i].wait()
        second[i].start()
    for copy in second:
        copy.wait()


def put_out(values):
    return pl.pallas_call(
        functools.partial(put_kernel, len(values)),
        out_shape=tuple(jax.ShapeDtypeStruct(v.shape, v.dtype) for v in values),
        in_specs=[HBM_SPEC] * len(values),
        out_specs=(HBM_SPEC,) * len(values),
        scratch_shapes=[pltpu.VMEM(v.shape, v.dtype) for v in values] + [DMA((2, len(values)))],
        compiler_params=pltpu.CompilerParams(vmem_limit_bytes=60 * 1024 * 1024),
        name="put_out",
    )(*values)


def local(tokens, cotangent, routes, route_weights, w_gate, w_up, w_down, dense_weight, mix_gate):
    token_grad, route_grad, gate_grad, up_grad, down_grad, dense_grad, mix_grad = put_out(layer(
        tokens, cotangent, routes.T, route_weights.T, dense_weight.T, mix_gate.reshape(1, -1),
        w_gate[0].T, w_up[0].T, w_down[0],
    ))
    return (
        token_grad, route_grad.T, gate_grad.T[None], up_grad.T[None], down_grad[None],
        dense_grad.T, mix_grad.reshape(-1),
    )


def solution(mesh):
    finer = Mesh(mesh.devices.reshape(NZ, NX, NC, NY), EP + ("y",))
    in_specs = (
        P(EP, "y"),
        P(EP, "y"),
        P(EP, None),
        P(EP, None),
        P(EP, None, "y"),
        P(EP, None, "y"),
        P(EP, "y", None),
        P("y", EP),
        P(),
    )
    out_specs = (
        P(EP, "y"),
        P(EP, None),
        P(EP, None, "y"),
        P(EP, None, "y"),
        P(EP, "y", None),
        P("y", EP),
        P(),
    )
    return jax.shard_map(local, mesh=finer, in_specs=in_specs, out_specs=out_specs, check_vma=False)
```

```python
import functools

import jax
import jax.numpy as jnp
from jax import lax
from jax.experimental import pallas as pl
from jax.experimental.pallas import tpu as pltpu
from jax.sharding import Mesh
from jax.sharding import PartitionSpec as P

EP = ("z", "x", "c")
MESH = pl.DeviceIdType.MESH
BF = jnp.bfloat16
F32 = jnp.float32
NZ = 16
NX = 4
NC = 2
NY = 4
CAP = 5
HK = NZ // NC
NQ = NX * NC
BLK = NQ * CAP
Z_ORDER = (0, 1, 7, 2, 6, 3, 5, 4)


def rdma(src, dst, send, recv, device):
    return pltpu.make_async_remote_copy(
        src_ref=src, dst_ref=dst, send_sem=send, recv_sem=recv, device_id=device, device_id_type=MESH
    )


def where_am_i():
    return tuple(lax.axis_index(a) for a in ("z", "x", "c", "y"))


def greet_all():
    z, x, c, y = where_am_i()
    barrier = pltpu.get_barrier_semaphore()

    def greet(device):
        pl.semaphore_signal(barrier, inc=1, device_id=device, device_id_type=MESH)

    for step in range(1, NQ):
        other = lax.rem(c * NX + x + step, NQ)
        greet((z, lax.rem(other, NX), other // NX, y))
    for step in range(1, NZ):
        greet((lax.rem(z + step, NZ), x, c, y))
    for step in range(1, NY):
        greet((z, x, c, lax.rem(y + step, NY)))


def wait_all():
    pl.semaphore_wait(pltpu.get_barrier_semaphore(), NQ - 1 + NZ - 1 + NY - 1)


def cols(index, width):
    return pl.ds(pl.multiple_of(index * width, width), width)


def permuted(perm_ref, value_ref, out_ref):
    width = value_ref.shape[-1]
    flat = value_ref[...].reshape(NQ * BLK, width)
    moved = jnp.dot(perm_ref[...], flat, preferred_element_type=F32).astype(BF)
    out_ref[...] = moved.reshape(NQ, BLK, width)


HALF = HK * BLK
LAG_F = 6
LAG_C = 12
PLAIN = (((1,), (0,)), ((), ()))
ROWS_BY = (((0,), (0,)), ((), ()))
COLS_BY = (((1,), (1,)), ((), ()))


def dot(a, b, dims):
    return lax.dot_general(a, b, dims, preferred_element_type=F32)


def gathered_rows(select, value_ref):
    rows = dot(select, value_ref[...], PLAIN).astype(BF)
    return rows.reshape(NQ, BLK, value_ref.shape[1])


def over_40(value):
    return (value * 52429) >> 21


def over_5(value):
    return (value * 52429) >> 18


def iota(shape, dim):
    return lax.broadcasted_iota(jnp.int32, shape, dim)


def ones_where(mask, dtype):
    return jnp.where(mask, 1.0, 0.0).astype(dtype)


def exact_dot(one_hot, value):
    high = value.astype(BF)
    low = (value - high.astype(F32)).astype(BF)
    return dot(one_hot, high, PLAIN) + dot(one_hot, low, PLAIN)


def layer_kernel(
    tokens_hbm, cot_hbm, routes_hbm, weights_hbm, wt_hbm, mix_hbm,
    wg_hbm, wu_hbm, wd_hbm,
    token_out, route_out, gate_out, up_out, down_out, dense_out, mix_out,
    *scratch,
):
    (
        s_tok, s_cot, x_tok, x_cot, p_tok, p_cot, rows_ref, grads_ref, wg, wu, wd, hid, dg, du,
        part, p_in, aux, aux_in, first, first_in, second_in, back, back_in, sorted_back, aux_sum,
        aux_y, aux_z, aux_t, moment_ref, m_in, m_half, m_x, m_xsum, m_z, g_mine, g_own, g_y,
        local_sem, x_send, x_recv, z_send, z_recv, yp_send, yp_recv, ym_send, ym_recv, f_send,
        f_recv, c_send, c_recv, g_send, g_recv, dz_send, dz_recv, dx_send, dx_recv, dc_send,
        dc_recv, mc_send, mc_recv, mx_send, mx_recv, mz_send, mz_recv, p_send, p_recv, b1_send,
        b1_recv, b2_send, b2_recv, ay_send, ay_recv, rz_send, rz_recv, rza_send, rza_recv, rx_send,
        rx_recv, rxa_send, rxa_recv, gy_send, gy_recv, gz_send, gz_recv, gx_send, gx_recv, gc_send,
        gc_recv,
        perm_ref, sel_ref, chosen_ref, full_ref, dense_ref, out_ref, aux_out, az_out, gain_out, pg, pu, dx_acc,
        gate_s, up_s, down_s, put_sem,
        tokens_ref, cot_ref, routes_ref, weights_ref, wt_ref, mix_ref, in_sem,
    ) = scratch
    z, x, c, y = where_am_i()
    width = tokens_ref.shape[-1]
    me_q = c * NX + x
    y_up, y_down = lax.rem(y + 1, NY), lax.rem(y + NY - 1, NY)
    y_far = lax.rem(y + 2, NY)
    partner = (z, x, 1 - c, y)
    slots = (s_tok, s_cot)
    gathered = (x_tok, x_cot)
    sorted_rows = (p_tok, p_cot)
    outs = (rows_ref, grads_ref)

    own = [
        pltpu.make_async_copy(cot_ref, full_ref.at[:, cols(y, width)], local_sem.at[0]),
        pltpu.make_async_copy(wt_ref, dense_ref.at[z, x, c], local_sem.at[1]),
    ]
    inputs = [
        pltpu.make_async_copy(source, target, in_sem.at[i])
        for i, (source, target) in enumerate((
            (routes_hbm, routes_ref), (weights_hbm, weights_ref), (tokens_hbm, tokens_ref),
            (cot_hbm, cot_ref), (wt_hbm, wt_ref), (mix_hbm, mix_ref),
        ))
    ]
    for copy in inputs:
        copy.start()
    weights = [
        pltpu.make_async_copy(wg_hbm, wg, local_sem.at[6]),
        pltpu.make_async_copy(wu_hbm, wu, local_sem.at[7]),
        pltpu.make_async_copy(wd_hbm, wd, local_sem.at[8]),
    ]
    for copy in weights:
        copy.start()
    greet_all()
    for copy in inputs:
        copy.wait()
    for copy in own:
        copy.start()
    table = (NQ * BLK, tokens_ref.shape[0])
    row = iota(table, 0)
    line = over_40(row)
    rest = row - BLK * line
    step_k = over_5(rest)
    slot = rest - CAP * step_k
    expert = ((z + 2 * step_k + (line >> 2)) & (NZ - 1)) * NX + (line & (NX - 1))
    hit_first = routes_ref[0:1, :] == expert
    hit_second = routes_ref[1:2, :] == expert
    square = (table[1], table[1])
    earlier = ones_where(iota(square, 0) < iota(square, 1), BF)
    hit = ones_where(hit_first, F32) + ones_where(hit_second, F32)
    rank = dot(hit.astype(BF), earlier, PLAIN)
    at_slot = ones_where(rank == slot.astype(F32), F32)
    chosen_ref[0] = ones_where(hit_first, F32) * at_slot
    chosen_ref[1] = ones_where(hit_second, F32) * at_slot
    gate_weights = weights_ref[...].astype(F32)
    select = (hit * at_slot).astype(BF)
    sel_ref[...] = select
    select_weighted = (chosen_ref[0] * gate_weights[0:1, :] + chosen_ref[1] * gate_weights[1:2, :]).astype(BF)
    slots[0][...] = gathered_rows(select, tokens_ref)
    slots[1][...] = gathered_rows(select_weighted, cot_ref)
    wait_all()

    def x_copy(a, step):
        other = lax.rem(me_q + step, NQ)
        return rdma(
            slots[a].at[other], gathered[a].at[me_q], x_send.at[a, step], x_recv.at[a, step],
            (z, lax.rem(other, NX), other // NX, y),
        )

    def x_arrival(a, step):
        source = lax.rem(me_q + NQ - step, NQ)
        return rdma(
            slots[a].at[source], gathered[a].at[source], x_send.at[a, step], x_recv.at[a, step],
            (z, lax.rem(source, NX), source // NX, y),
        )

    for a in range(2):
        for step in range(1, NQ):
            x_copy(a, step).start()

    def g_copy(step):
        return rdma(
            cot_ref, full_ref.at[:, cols(y, width)], g_send.at[step], g_recv.at[step],
            (z, x, c, lax.rem(y + step, NY)),
        )

    def g_arrival(step):
        source = lax.rem(y + NY - step, NY)
        return rdma(
            cot_ref, full_ref.at[:, cols(source, width)], g_send.at[step], g_recv.at[step],
            (z, x, c, source),
        )

    for step in range(1, NY):
        g_copy(step).start()

    def dz_copy(step):
        return rdma(
            wt_ref, dense_ref.at[z, x, c], dz_send.at[step], dz_recv.at[step],
            (lax.rem(z + step, NZ), x, c, y),
        )

    def dz_arrival(step):
        source = lax.rem(z + NZ - step, NZ)
        return rdma(
            wt_ref, dense_ref.at[source, x, c], dz_send.at[step], dz_recv.at[step], (source, x, c, y)
        )

    @pl.loop(1, NZ)
    def _(step):
        dz_copy(step).start()

    both_ways = (NQ * BLK, NQ * BLK)
    place = iota(both_ways, 0)
    block = over_40(place)
    inside = place - BLK * block
    source = over_5(inside)
    perm_ref[...] = ones_where(
        source * BLK + block * CAP + (inside - CAP * source) == iota(both_ways, 1), BF
    )

    def z_copy(a, k):
        target = lax.rem(z + 2 * k + c, NZ)
        return rdma(
            sorted_rows[a].at[k], outs[a].at[c * HK + k, :, cols(y, width)],
            z_send.at[a, k], z_recv.at[a, k], (target, x, c, y),
        )

    def z_home(a):
        return pltpu.make_async_copy(
            sorted_rows[a].at[0], outs[a].at[0, :, cols(y, width)], local_sem.at[2 + a]
        )

    for a in range(2):
        gathered[a][me_q] = slots[a][me_q]
        for step in range(1, NQ):
            x_arrival(a, step).wait_recv()
        permuted(perm_ref, gathered[a], sorted_rows[a])
        for k in Z_ORDER:
            if k == 0:

                @pl.when(c == 0)
                def _():
                    z_home(a).start()

                @pl.when(c == 1)
                def _():
                    z_copy(a, 0).start()
            else:
                z_copy(a, k).start()

    def y_copy(a, k, up):
        part = outs[a].at[c * HK + k, :, cols(y, width)]
        if up:
            return rdma(part, part, yp_send.at[a, k], yp_recv.at[a, k], (z, x, c, y_up))
        return rdma(part, part, ym_send.at[a, k], ym_recv.at[a, k], (z, x, c, y_down))

    def y_arrival(a, k, up):
        if up:
            part = outs[a].at[c * HK + k, :, cols(y_down, width)]
            return rdma(part, part, yp_send.at[a, k], yp_recv.at[a, k], (z, x, c, y_down))
        part = outs[a].at[c * HK + k, :, cols(y_up, width)]
        return rdma(part, part, ym_send.at[a, k], ym_recv.at[a, k], (z, x, c, y_up))

    def f_copy(a, k):
        source, target = (y_down, y_up) if k % 2 == 0 else (y_up, y_down)
        part = outs[a].at[c * HK + k, :, cols(source, width)]
        return rdma(part, part, f_send.at[a, k], f_recv.at[a, k], (z, x, c, target))

    def f_arrival(a, k):
        part = outs[a].at[c * HK + k, :, cols(y_far, width)]
        return rdma(part, part, f_send.at[a, k], f_recv.at[a, k], (z, x, c, y_up))

    def c_copy(a, k):
        block = outs[a].at[c * HK + k]
        return rdma(block, block, c_send.at[a, k], c_recv.at[a, k], partner)

    def c_arrival(a, k):
        block = outs[a].at[(1 - c) * HK + k]
        return rdma(block, block, c_send.at[a, k], c_recv.at[a, k], partner)

    def dx_copy(step):
        part = dense_ref.at[:, x, c]
        return rdma(part, part, dx_send.at[step], dx_recv.at[step], (z, lax.rem(x + step, NX), c, y))

    def dx_arrival(step):
        source = lax.rem(x + NX - step, NX)
        part = dense_ref.at[:, source, c]
        return rdma(part, part, dx_send.at[step], dx_recv.at[step], (z, source, c, y))

    def dc_copy(core):
        part = dense_ref.at[:, :, core]
        return rdma(part, part, dc_send.at[0], dc_recv.at[0], partner)

    own[0].wait()
    for step in range(1, NY):
        g_arrival(step).wait_recv()
    moment_ref[...] = dot(full_ref[...], tokens_ref[...], ROWS_BY).reshape(moment_ref.shape)

    def mc_copy():
        return rdma(moment_ref.at[:, :, 1 - c], m_in, mc_send.at[0], mc_recv.at[0], partner)

    mc_copy().start()

    def mx_copy(step):
        other = lax.rem(x + step, NX)
        return rdma(m_half.at[:, other], m_x.at[step - 1], mx_send.at[step], mx_recv.at[step],
                    (z, other, c, y))

    def mz_copy(step):
        other = lax.rem(z + step, NZ)
        return rdma(m_xsum.at[other], m_z.at[step], mz_send.at[step], mz_recv.at[step],
                    (other, x, c, y))

    def rows_of(ref, turn):
        group = jnp.where(turn == 0, 1 - c, c)
        return ref[pl.ds(group * HK, HK)].reshape(HALF, NY * width)

    order = [(a, k) for a in range(2) for k in Z_ORDER]
    for i in range(len(order) + LAG_C):
        if i < len(order):
            a, k = order[i]
            if k == 0:

                @pl.when(c == 0)
                def _():
                    z_home(a).wait()

                @pl.when(c == 1)
                def _():
                    z_copy(a, 0).wait_recv()
            else:
                z_copy(a, k).wait_recv()
            y_copy(a, k, True).start()
            y_copy(a, k, False).start()
        if LAG_F <= i < len(order) + LAG_F:
            a, k = order[i - LAG_F]
            up = k % 2 == 0
            y_arrival(a, k, up).wait_recv()
            f_copy(a, k).start()
            y_arrival(a, k, not up).wait_recv()
        if i >= LAG_C:
            a, k = order[i - LAG_C]
            f_arrival(a, k).wait_recv()
            c_copy(a, k).start()
        if i == 6:
            own[1].wait()

            @pl.loop(1, NZ)
            def _(step):
                dz_arrival(step).wait_recv()

            for step in range(1, NX):
                dx_copy(step).start()
        if i == 8:
            mc_copy().wait_recv()
            for n in range(NX):
                m_half[:, n] = moment_ref[:, n, c] + m_in[:, n]
            for step in range(1, NX):
                mx_copy(step).start()
        if i == 19:
            for copy in weights:
                copy.wait()
            for k in Z_ORDER:
                c_arrival(0, k).wait_recv()
        if 20 <= i < 24:
            turn = (i - 20) // 2
            if i % 2 == 0:
                pg[turn] = dot(rows_of(rows_ref, turn), wg[...], COLS_BY)
            else:
                pu[turn] = dot(rows_of(rows_ref, turn), wu[...], COLS_BY)
        if i == 20:
            for step in range(1, NX):
                mx_copy(step).wait_recv()
            m_xsum[...] = (m_half[:, x] + m_x[0] + m_x[1] + m_x[2]).astype(BF)

            @pl.loop(1, NZ)
            def _(step):
                mz_copy(step).start()
        if i == 12:
            for step in range(1, NX):
                dx_arrival(step).wait_recv()
            dc_copy(c).start()

    dc_copy(1 - c).wait_recv()
    for k in Z_ORDER:
        c_arrival(1, k).wait_recv()

    def p_copy():
        return rdma(part.at[0], p_in, p_send.at[0], p_recv.at[0], partner)

    def pa_copy():
        return rdma(aux.at[0], aux_in, p_send.at[1], p_recv.at[1], partner)

    @pl.loop(0, 2)
    def _(turn):
        pre_gate = pg[turn]
        pre_up = pu[turn]
        back_h = dot(rows_of(grads_ref, turn), wd[...], COLS_BY)
        sig = jax.nn.sigmoid(pre_gate)
        act = pre_gate * sig
        hidden_bf = (act * pre_up).astype(BF)
        hid[turn] = hidden_bf
        d_gate = (back_h * pre_up * sig * (1.0 + pre_gate * (1.0 - sig))).astype(BF)
        d_up = (back_h * act).astype(BF)
        dg[turn] = d_gate
        du[turn] = d_up
        route = jnp.sum(hidden_bf.astype(F32) * back_h, axis=1, keepdims=True)
        at = (HALF, 128)
        lane_is = over_40(iota(at, 0)) * -BLK + iota(at, 0) == iota(at, 1)
        block_of = ones_where(over_40(iota((HK, HALF), 1)) == iota((HK, HALF), 0), BF)
        aux[turn] = exact_dot(block_of, jnp.where(lane_is, route, 0.0))
        both_parts = dot(d_gate, wg[...], PLAIN) + dot(d_up, wu[...], PLAIN)
        part[turn] = both_parts.astype(BF).reshape(HK, BLK, NY * width)

        @pl.when(turn == 0)
        def _():
            p_copy().start()
            pa_copy().start()

    half = HK // 2
    flip1 = y + 1 - 2 * lax.rem(y, 2)
    flip3 = NY - 1 - y
    flip2 = lax.rem(y + 2, NY)
    pairs = ((flip1, flip3), (flip3, flip1))

    p_copy().wait_recv()

    def b1_copy(h):
        return rdma(
            first.at[h, pl.ds(2, 2)], first_in.at[h], b1_send.at[h], b1_recv.at[h],
            (z, x, c, pairs[h][0]),
        )

    def both(h, i, owner):
        for j in range(half):
            mine = part[1, h * half + j, :, cols(owner, width)].astype(F32)
            theirs = p_in[h * half + j, :, cols(owner, width)].astype(F32)
            first[h, i, j] = (mine + theirs).astype(BF)

    for h in range(2):
        both(h, 2, pairs[h][0])
        both(h, 3, flip2)
        b1_copy(h).start()
    for h in range(2):
        both(h, 0, y)
        both(h, 1, pairs[h][1])

    pa_copy().wait_recv()
    aux_sum[...] = aux[1] + aux_in[...]

    def ay_copy(step):
        return rdma(aux_sum, aux_y.at[y], ay_send.at[step], ay_recv.at[step],
                    (z, x, c, lax.rem(y + step, NY)))

    def ay_arrival(step):
        source = lax.rem(y + NY - step, NY)
        return rdma(aux_sum, aux_y.at[source], ay_send.at[step], ay_recv.at[step], (z, x, c, source))

    for step in range(1, NY):
        ay_copy(step).start()
    aux_y[y] = aux_sum[...]

    def b2_copy(h):
        return rdma(first.at[h, 3], second_in.at[h], b2_send.at[h], b2_recv.at[h],
                    (z, x, c, pairs[h][1]))

    for h in range(2):
        b1_copy(h).wait()
        first[h, 3] = (first[h, 1].astype(F32) + first_in[h, 1].astype(F32)).astype(BF)
        b2_copy(h).start()

    for step in range(1, NY):
        ay_arrival(step).wait_recv()
        ay_copy(step).wait_send()
    aux_sum[...] = aux_y[0] + aux_y[1] + aux_y[2] + aux_y[3]
    for k in range(HK):
        az_out[k] = aux_sum[k : k + 1]

    def r_z_copy(k):
        target = lax.rem(z + 2 * NZ - 2 * k - c, NZ)
        return rdma(back.at[k], back_in.at[k], rz_send.at[k], rz_recv.at[k], (target, x, c, y))

    def r_za_copy(k):
        target = lax.rem(z + 2 * NZ - 2 * k - c, NZ)
        return rdma(az_out.at[k], aux_z.at[k], rza_send.at[k], rza_recv.at[k], (target, x, c, y))

    r_z_home = [
        pltpu.make_async_copy(back.at[0], back_in.at[0], local_sem.at[4]),
        pltpu.make_async_copy(az_out.at[0], aux_z.at[0], local_sem.at[5]),
    ]

    def send_back(k):
        if k == 0:

            @pl.when(c == 0)
            def _():
                r_z_home[0].start()
                r_z_home[1].start()

            @pl.when(c == 1)
            def _():
                r_z_copy(0).start()
                r_za_copy(0).start()
        else:
            r_z_copy(k).start()
            r_za_copy(k).start()

    for h in range(2):
        b2_copy(h).wait()
        back[pl.ds(h * half, half)] = (
            first[h, 0].astype(F32) + first_in[h, 0].astype(F32) + second_in[h].astype(F32)
        ).astype(BF)
    for k in reversed(Z_ORDER):
        send_back(k)

    m_z[0] = m_xsum[z]

    @pl.loop(1, NZ)
    def _(step):
        mz_copy(step).wait()

    moment_own = jnp.sum(m_z[...].astype(F32), axis=0)
    ep_index = (z * NX + x) * NC + c
    here = (moment_own.shape[0], NY * width)
    is_own = iota(here, 1) == ep_index * here[0] + iota(here, 0)
    own_gate = jnp.sum(jnp.where(is_own, mix_ref[...], 0.0), axis=1, keepdims=True)
    dense_out[...] = moment_own * (own_gate * (1.0 / (NZ * NX * NC)))
    gain = jnp.sum(wt_ref[...].astype(F32) * moment_own, axis=1, keepdims=True)
    g_mine[...] = jnp.broadcast_to(gain, g_mine.shape)

    def gy_copy(step):
        return rdma(g_mine, g_y.at[y], gy_send.at[step], gy_recv.at[step],
                    (z, x, c, lax.rem(y + step, NY)))

    def gy_arrival(step):
        source = lax.rem(y + NY - step, NY)
        return rdma(g_mine, g_y.at[source], gy_send.at[step], gy_recv.at[step], (z, x, c, source))

    for step in range(1, NY):
        gy_copy(step).start()
    g_y[y] = g_mine[...]

    puts = [
        pltpu.make_async_copy(source, target, put_sem.at[i])
        for i, (source, target) in enumerate(((gate_s, gate_out), (up_s, up_out), (down_s, down_out)))
    ]

    def over_rows(a, b):
        return dot(a, b, ROWS_BY)

    down_s[...] = (
        over_rows(hid[0], rows_of(grads_ref, 0)) + over_rows(hid[1], rows_of(grads_ref, 1))
    ).astype(BF)
    puts[2].start()
    for step in range(1, NY):
        gy_arrival(step).wait_recv()
    g_own[...] = g_y[0] + g_y[1] + g_y[2] + g_y[3]

    def gz_copy(step):
        return rdma(g_own, gain_out.at[z, x, c], gz_send.at[step], gz_recv.at[step],
                    (lax.rem(z + step, NZ), x, c, y))

    def gz_arrival(step):
        source = lax.rem(z + NZ - step, NZ)
        return rdma(g_own, gain_out.at[source, x, c], gz_send.at[step], gz_recv.at[step],
                    (source, x, c, y))

    @pl.loop(1, NZ)
    def _(step):
        gz_copy(step).start()

    gain_out[z, x, c] = g_own[...]

    gate_s[...] = (
        over_rows(dg[0], rows_of(rows_ref, 0)) + over_rows(dg[1], rows_of(rows_ref, 1))
    ).astype(BF)
    puts[0].start()
    up_s[...] = (
        over_rows(du[0], rows_of(rows_ref, 0)) + over_rows(du[1], rows_of(rows_ref, 1))
    ).astype(BF)
    puts[1].start()
    scaled = (mix_ref[...] * full_ref[...].astype(F32)).astype(BF)
    dx_acc[...] = dot(scaled, dense_ref[...].reshape(NY * width, width), PLAIN)

    @pl.loop(1, NZ)
    def _(step):
        gz_arrival(step).wait_recv()

    def gx_copy(step):
        tiles = gain_out.at[:, x, c]
        return rdma(tiles, tiles, gx_send.at[step], gx_recv.at[step], (z, lax.rem(x + step, NX), c, y))

    def gx_arrival(step):
        source = lax.rem(x + NX - step, NX)
        tiles = gain_out.at[:, source, c]
        return rdma(tiles, tiles, gx_send.at[step], gx_recv.at[step], (z, source, c, y))

    for step in range(1, NX):
        gx_copy(step).start()

    def gc_copy(core):
        tiles = gain_out.at[:, :, core]
        return rdma(tiles, tiles, gc_send.at[0], gc_recv.at[0], partner)

    for k in Z_ORDER:
        if k == 0:

            @pl.when(c == 0)
            def _():
                r_z_home[0].wait()
                r_z_home[1].wait()

            @pl.when(c == 1)
            def _():
                r_z_copy(0).wait()
                r_za_copy(0).wait()
        else:
            r_z_copy(k).wait()
            r_za_copy(k).wait()
    permuted(perm_ref, back_in, sorted_back)
    for k in range(HK):
        aux_t[k : k + 1] = aux_z[k]

    def r_x_copy(step):
        other = lax.rem(me_q + step, NQ)
        return rdma(sorted_back.at[other], out_ref.at[me_q], rx_send.at[step], rx_recv.at[step],
                    (z, lax.rem(other, NX), other // NX, y))

    def r_xa_copy(step):
        other = lax.rem(me_q + step, NQ)
        return rdma(aux_t, aux_out.at[me_q], rxa_send.at[step], rxa_recv.at[step],
                    (z, lax.rem(other, NX), other // NX, y))

    def r_x_arrival(step):
        source = lax.rem(me_q + NQ - step, NQ)
        device = (z, lax.rem(source, NX), source // NX, y)
        return (
            rdma(sorted_back.at[source], out_ref.at[source], rx_send.at[step], rx_recv.at[step], device),
            rdma(aux_t, aux_out.at[source], rxa_send.at[step], rxa_recv.at[step], device),
        )

    for step in range(1, NQ):
        r_x_copy(step).start()
        r_xa_copy(step).start()
    out_ref[me_q] = sorted_back[me_q]
    aux_out[me_q] = aux_t[...]

    for step in range(1, NX):
        gx_arrival(step).wait_recv()
    gc_copy(c).start()
    gc_copy(1 - c).wait_recv()
    for step in range(1, NQ):
        for arrival in r_x_arrival(step):
            arrival.wait_recv()
    token_out[...] = (
        dx_acc[...] + dot(sel_ref[...], out_ref[...].reshape(NQ * BLK, width), ROWS_BY)
    ).astype(BF)
    group_of = ones_where(over_5(iota((NQ * BLK, HK * NQ), 0)) == iota((NQ * BLK, HK * NQ), 1), BF)
    values = exact_dot(group_of, aux_out[...].reshape(HK * NQ, 128))
    at = (NQ * BLK, 128)
    lane_is = iota(at, 0) - CAP * over_5(iota(at, 0)) + me_q * CAP == iota(at, 1)
    value = jnp.sum(jnp.where(lane_is, values, 0.0), axis=1, keepdims=True)
    home_weights = weights_ref[...].astype(F32)
    for p in range(2):
        total = jnp.sum(chosen_ref[p] * value, axis=0, keepdims=True)
        route_out[p : p + 1, :] = total / home_weights[p : p + 1, :]
    tiles_in = gain_out[...].reshape(NZ * NX * NC * here[0], 128)
    diagonal = ones_where(iota((128, 128), 0) == iota((128, 128), 1), F32)
    for n in range(NZ * NX * NC * here[0] // 128):
        picked = jnp.sum(tiles_in[n * 128 : (n + 1) * 128] * diagonal, axis=0, keepdims=True)
        mix_out[n : n + 1, :] = picked * (1.0 / (NZ * NX * NC))
    for copy in puts:
        copy.wait()
    for step in range(1, NQ):
        r_x_copy(step).wait_send()
        r_xa_copy(step).wait_send()
    p_copy().wait_send()
    pa_copy().wait_send()
    gc_copy(c).wait_send()
    for step in range(1, NX):
        gx_copy(step).wait_send()
    for step in range(1, NY):
        gy_copy(step).wait_send()

    @pl.loop(1, NZ)
    def _(step):
        gz_copy(step).wait_send()

    for a in range(2):
        for step in range(1, NQ):
            x_copy(a, step).wait_send()
    for step in range(1, NY):
        g_copy(step).wait_send()

    @pl.loop(1, NZ)
    def _(step):
        dz_copy(step).wait_send()

    for step in range(1, NX):
        dx_copy(step).wait_send()
    dc_copy(c).wait_send()
    for a, k in order:
        if k == 0:

            @pl.when(c == 1)
            def _():
                z_copy(a, 0).wait_send()
        else:
            z_copy(a, k).wait_send()
        y_copy(a, k, True).wait_send()
        y_copy(a, k, False).wait_send()
        f_copy(a, k).wait_send()
        c_copy(a, k).wait_send()
    mc_copy().wait_send()
    for step in range(1, NX):
        mx_copy(step).wait_send()


VMEM_SPEC = pl.BlockSpec(memory_space=pltpu.VMEM)
HBM_SPEC = pl.BlockSpec(memory_space=pl.ANY)
DMA = pltpu.SemaphoreType.DMA


def layer(tokens, cotangent, routes, weights, wt, mix_gate, gate, up, down):
    width = tokens.shape[1]
    half = HK // 2
    own = wt.shape[0]
    hidden = gate.shape[0]
    vm = pltpu.VMEM
    shape = jax.ShapeDtypeStruct
    return pl.pallas_call(
        layer_kernel,
        out_shape=(
            shape(tokens.shape, BF),
            shape(routes.shape, F32),
            shape(gate.shape, BF),
            shape(up.shape, BF),
            shape(down.shape, BF),
            shape(wt.shape, F32),
            shape((NY * width // 128, 128), F32),
        ),
        in_specs=[HBM_SPEC] * 9,
        out_specs=(VMEM_SPEC,) * 2 + (HBM_SPEC,) * 3 + (VMEM_SPEC,) * 2,
        scratch_shapes=[
            vm((NQ, BLK, width), BF),
            vm((NQ, BLK, width), BF),
            vm((NQ, BLK, width), BF),
            vm((NQ, BLK, width), BF),
            vm((NQ, BLK, width), BF),
            vm((NQ, BLK, width), BF),
            vm((NZ, BLK, NY * width), BF),
            vm((NZ, BLK, NY * width), BF),
            vm(gate.shape, BF),
            vm(gate.shape, BF),
            vm(down.shape, BF),
            vm((2, HALF, hidden), BF),
            vm((2, HALF, hidden), BF),
            vm((2, HALF, hidden), BF),
            vm((2, HK, BLK, NY * width), BF),
            vm((HK, BLK, NY * width), BF),
            vm((2, HK, 128), F32),
            vm((HK, 128), F32),
            vm((2, NY, half, BLK, width), BF),
            vm((2, 2, half, BLK, width), BF),
            vm((2, half, BLK, width), BF),
            vm((HK, BLK, width), BF),
            vm((HK, BLK, width), BF),
            vm((NQ, BLK, width), BF),
            vm((HK, 128), F32),
            vm((NY, HK, 128), F32),
            vm((HK, 1, 128), F32),
            vm((HK, 128), F32),
            vm((NZ, NX, NC, own, width), F32),
            vm((NZ, NX, own, width), F32),
            vm((NZ, NX, own, width), F32),
            vm((NX - 1, NZ, own, width), F32),
            vm((NZ, own, width), BF),
            vm((NZ, own, width), BF),
            vm((own, 128), F32),
            vm((own, 128), F32),
            vm((NY, own, 128), F32),
            DMA((9,)),
            DMA((2, NQ)),
            DMA((2, NQ)),
            DMA((2, HK)),
            DMA((2, HK)),
            DMA((2, HK)),
            DMA((2, HK)),
            DMA((2, HK)),
            DMA((2, HK)),
            DMA((2, HK)),
            DMA((2, HK)),
            DMA((2, HK)),
            DMA((2, HK)),
            DMA((NY,)),
            DMA((NY,)),
            DMA((NZ,)),
            DMA((NZ,)),
            DMA((NX,)),
            DMA((NX,)),
            DMA((1,)),
            DMA((1,)),
            DMA((1,)),
            DMA((1,)),
            DMA((NX,)),
            DMA((NX,)),
            DMA((NZ,)),
            DMA((NZ,)),
            DMA((2,)),
            DMA((2,)),
            DMA((2,)),
            DMA((2,)),
            DMA((2,)),
            DMA((2,)),
            DMA((NY,)),
            DMA((NY,)),
            DMA((HK,)),
            DMA((HK,)),
            DMA((HK,)),
            DMA((HK,)),
            DMA((NQ,)),
            DMA((NQ,)),
            DMA((NQ,)),
            DMA((NQ,)),
            DMA((NY,)),
            DMA((NY,)),
            DMA((NZ,)),
            DMA((NZ,)),
            DMA((NX,)),
            DMA((NX,)),
            DMA((1,)),
            DMA((1,)),
            vm((NQ * BLK, NQ * BLK), BF),
            vm((NQ * BLK, tokens.shape[0]), BF),
            vm((2, NQ * BLK, tokens.shape[0]), F32),
            vm((tokens.shape[0], NY * width), BF),
            vm((NZ, NX, NC) + wt.shape, BF),
            vm((NQ, BLK, width), BF),
            vm((NQ, HK, 128), F32),
            vm((HK, 1, 128), F32),
            vm((NZ, NX, NC, own, 128), F32),
            vm((2, HALF, hidden), F32),
            vm((2, HALF, hidden), F32),
            vm(tokens.shape, F32),
            vm(gate.shape, BF),
            vm(gate.shape, BF),
            vm(down.shape, BF),
            DMA((3,)),
            vm(tokens.shape, BF),
            vm(tokens.shape, BF),
            vm(routes.shape, jnp.int32),
            vm(weights.shape, BF),
            vm(wt.shape, BF),
            vm(mix_gate.shape, F32),
            DMA((6,)),
        ],
        compiler_params=pltpu.CompilerParams(
            collective_id=0, has_side_effects=True, vmem_limit_bytes=60 * 1024 * 1024
        ),
        name="layer",
    )(tokens, cotangent, routes, weights, wt, mix_gate, gate, up, down)


def put_kernel(count, *refs):
    ins, outs, held, sems = refs[:count], refs[count : 2 * count], refs[2 * count : -1], refs[-1]
    first = [pltpu.make_async_copy(ins[i], held[i], sems.at[0, i]) for i in range(count)]
    second = [pltpu.make_async_copy(held[i], outs[i], sems.at[1, i]) for i in range(count)]
    for copy in first:
        copy.start()
    for i in range(count):
        first[i].wait()
        second[i].start()
    for copy in second:
        copy.wait()


def put_out(values):
    return pl.pallas_call(
        functools.partial(put_kernel, len(values)),
        out_shape=tuple(jax.ShapeDtypeStruct(v.shape, v.dtype) for v in values),
        in_specs=[HBM_SPEC] * len(values),
        out_specs=(HBM_SPEC,) * len(values),
        scratch_shapes=[pltpu.VMEM(v.shape, v.dtype) for v in values] + [DMA((2, len(values)))],
        compiler_params=pltpu.CompilerParams(vmem_limit_bytes=60 * 1024 * 1024),
        name="put_out",
    )(*values)


def local(tokens, cotangent, routes, route_weights, w_gate, w_up, w_down, dense_weight, mix_gate):
    token_grad, route_grad, gate_grad, up_grad, down_grad, dense_grad, mix_grad = put_out(layer(
        tokens, cotangent, routes.T, route_weights.T, dense_weight.T, mix_gate.reshape(1, -1),
        w_gate[0].T, w_up[0].T, w_down[0],
    ))
    return (
        token_grad, route_grad.T, gate_grad.T[None], up_grad.T[None], down_grad[None],
        dense_grad.T, mix_grad.reshape(-1),
    )


def solution(mesh):
    finer = Mesh(mesh.devices.reshape(NZ, NX, NC, NY), EP + ("y",))
    in_specs = (
        P(EP, "y"),
        P(EP, "y"),
        P(EP, None),
        P(EP, None),
        P(EP, None, "y"),
        P(EP, None, "y"),
        P(EP, "y", None),
        P("y", EP),
        P(),
    )
    out_specs = (
        P(EP, "y"),
        P(EP, None),
        P(EP, None, "y"),
        P(EP, None, "y"),
        P(EP, "y", None),
        P("y", EP),
        P(),
    )
    return jax.shard_map(local, mesh=finer, in_specs=in_specs, out_specs=out_specs, check_vma=False)
```
